512 devices in a mesh: sp: 64 (over z, y), tp: 8 (over x, core).
Axes of the slice: x: 4, y: 8, z: 8, core: 2. Of those that a mesh axis runs over, the one named last changes fastest.
Arguments:
- queries: bfloat16 [1, 24576, 2048], P(None, 'sp', 'tp'), may hold values from -5 to 5
- keys: bfloat16 [1, 24576, 2048], P(None, 'sp', 'tp'), may hold values from -5 to 5
- values: bfloat16 [1, 24576, 2048], P(None, 'sp', 'tp'), may hold values from -6 to 6
- rel_bias: float32 [16, 192], P('tp'), may hold values from -3 to 3
- out_grad: bfloat16 [1, 24576, 2048], P(None, 'sp', 'tp'), may hold values from -48 to 48
Outputs:
- query_grad: bfloat16 [1, 24576, 2048], P(None, 'sp', 'tp')
- key_grad: bfloat16 [1, 24576, 2048], P(None, 'sp', 'tp')
- value_grad: bfloat16 [1, 24576, 2048], P(None, 'sp', 'tp')
- bias_grad: float32 [16, 192], replicated
The draws below stay inside these ranges and needn't reach their ends.
All inputs are finite; a program needn't handle non-finite values.
Results may differ from the reference program's by a relative error of at most 0.0049.
Values may be sent and summed in bfloat16 or wider, within the bound.
A program may use at most 64 MiB of HBM per device.

```python
import jax
import jax.numpy as jnp
from jax import lax

HEADS = 16
HEAD_DIM = 128
SEG = 64
LEFT = 4
CLIP = 128
SEQS = 1
TOK_DEV = 384
LENGTH = 24576
WIDTH = 2048
BAND = 320
BUCKETS = 192


def aligned_pair(key):
    shape = (SEQS, LENGTH, HEADS * HEAD_DIM)
    base_q = jax.random.normal(jax.random.fold_in(key, 11), shape, jnp.float32)
    base_k = jax.random.normal(jax.random.fold_in(key, 12), shape, jnp.float32)
    return (jnp.clip(base_q, -5.0, 5.0), jnp.clip(base_k, -5.0, 5.0))


def draw_queries(key, part):
    return aligned_pair(key)[0].astype(jnp.bfloat16)


def draw_keys(key, part):
    return aligned_pair(key)[1].astype(jnp.bfloat16)


def steps_of(own_key, dims, pieces, smallest, high):
    def one(dim, blocks):
        heights = jax.random.uniform(jax.random.fold_in(jax.random.fold_in(own_key, 6), dim), (blocks,), jnp.float32, smallest / len(pieces), high / len(pieces))
        return jnp.repeat(jnp.exp(heights), dims[dim] // blocks).reshape((-1,) + (1,) * (len(dims) - dim - 1))

    gain = one(*pieces[0])
    for cut in pieces[1:]:
        gain = gain * one(*cut)
    return gain


def gaussian(rng, shape, width, limit, shards=(), held_as=jnp.bfloat16):
    factor_of = steps_of(rng, shape, shards, -0.22, 0.18) if shards else 1.0
    drawn = jax.random.normal(rng, shape, jnp.float32) * width * factor_of
    return jnp.minimum(jnp.maximum(drawn, -limit), limit).astype(held_as)


def setup_inputs(seed: int = 0) -> dict:
    arg_keys = jax.random.split(jax.random.key(seed), 6)
    queries = draw_queries(jax.random.fold_in(arg_keys[5], 71), 0)
    keys = draw_keys(jax.random.fold_in(arg_keys[5], 71), 0)
    values = gaussian(arg_keys[2], (SEQS, LENGTH, WIDTH), 1.0, 6.0, ((1, 64), (2, 8)))
    rel_bias = gaussian(arg_keys[3], (HEADS, BUCKETS), 0.5, 3.0, ((0, 8),), jnp.float32)
    out_grad = gaussian(arg_keys[4], (SEQS, LENGTH, WIDTH), 8.0, 48.0, ((1, 64), (2, 8)))
    return dict(queries=queries, keys=keys, values=values, rel_bias=rel_bias, out_grad=out_grad)


def relative_index():
    rows = jnp.arange(SEG, dtype=jnp.int32)[:, None] + LEFT * SEG
    cols = jnp.arange(BAND, dtype=jnp.int32)[None, :]
    return (jnp.clip(rows - cols, 1 - SEG, CLIP) + SEG - 1).astype(jnp.int32)


def low_round(array):
    return lax.optimization_barrier(array.astype(jnp.bfloat16)).astype(jnp.float32)


def band_math(q_segs, k_band, v_band, g_segs, table, key_valid):
    seg_count = q_segs.shape[1]
    score_scale = HEAD_DIM ** -0.5
    q_full = q_segs.astype(jnp.float32)
    g_full = g_segs.astype(jnp.float32)
    k_full = k_band.astype(jnp.float32)
    v_full = v_band.astype(jnp.float32)
    score_parts = []
    prob_parts = []
    for offset in range(LEFT + 1):
        score_parts.append(jnp.einsum('sncha,snkha->snhck', q_full, k_full[:, offset:offset + seg_count]))
        prob_parts.append(jnp.einsum('sncha,snkha->snhck', g_full, v_full[:, offset:offset + seg_count]))
    score = jnp.concatenate(score_parts, axis=-1) * score_scale + table[None, None]
    score = jnp.where(key_valid[None, :, None, None, :], score, -jnp.inf)
    row_max = jnp.max(score, axis=-1, keepdims=True)
    expo = jnp.exp(score - row_max)
    prob = expo / jnp.sum(expo, axis=-1, keepdims=True)
    prob_grad = jnp.concatenate(prob_parts, axis=-1)
    row_delta = jnp.sum(prob * prob_grad, axis=-1, keepdims=True)
    score_grad = prob * (prob_grad - row_delta)
    bias_terms = jnp.sum(score_grad, axis=(0, 1))
    prob_low = low_round(prob)
    grad_low = low_round(score_grad * score_scale)
    query_acc = jnp.zeros(q_full.shape, jnp.float32)
    key_acc = jnp.zeros(k_full.shape, jnp.float32)
    value_acc = jnp.zeros(k_full.shape, jnp.float32)
    for offset in range(LEFT + 1):
        grad_part = grad_low[..., offset * SEG:(offset + 1) * SEG]
        prob_part = prob_low[..., offset * SEG:(offset + 1) * SEG]
        query_acc = query_acc + jnp.einsum('snhck,snkha->sncha', grad_part, k_full[:, offset:offset + seg_count])
        key_acc = key_acc.at[:, offset:offset + seg_count].add(jnp.einsum('snhck,sncha->snkha', grad_part, q_full))
        value_acc = value_acc.at[:, offset:offset + seg_count].add(jnp.einsum('snhck,sncha->snkha', prob_part, g_full))
    return query_acc, key_acc, value_acc, bias_terms


def reference(queries, keys, values, rel_bias, out_grad):
    seq_count, length, row_width = queries.shape
    head_count = row_width // HEAD_DIM
    reach = LEFT * SEG
    block_rows = TOK_DEV
    seg_count = block_rows // SEG
    zero_rows = jnp.zeros((seq_count, reach, row_width), keys.dtype)
    keys_pad = jnp.concatenate([zero_rows, keys], axis=1)
    values_pad = jnp.concatenate([zero_rows, values], axis=1)
    rel_ids = relative_index()
    table = jnp.take(rel_bias.astype(jnp.float32), rel_ids, axis=1)
    seg_shape = (seq_count, seg_count, SEG, head_count, HEAD_DIM)
    band_shape = (seq_count, seg_count + LEFT, SEG, head_count, HEAD_DIM)

    def step(carry, block):
        key_sum, value_sum, bias_sum = carry
        start = (block * block_rows).astype(jnp.int32)
        q_blk = lax.dynamic_slice_in_dim(queries, start, block_rows, 1).reshape(seg_shape)
        g_blk = lax.dynamic_slice_in_dim(out_grad, start, block_rows, 1).reshape(seg_shape)
        k_blk = lax.dynamic_slice_in_dim(keys_pad, start, block_rows + reach, 1).reshape(band_shape)
        v_blk = lax.dynamic_slice_in_dim(values_pad, start, block_rows + reach, 1).reshape(band_shape)
        positions = start + jnp.arange(seg_count, dtype=jnp.int32)[:, None] * SEG - reach + jnp.arange(BAND, dtype=jnp.int32)[None, :]
        key_valid = positions >= 0
        query_acc, key_acc, value_acc, bias_terms = band_math(q_blk, k_blk, v_blk, g_blk, table, key_valid)
        flat = (seq_count, block_rows + reach, row_width)
        key_sum = lax.dynamic_update_slice_in_dim(key_sum, lax.dynamic_slice_in_dim(key_sum, start, block_rows + reach, 1) + key_acc.reshape(flat), start, 1)
        value_sum = lax.dynamic_update_slice_in_dim(value_sum, lax.dynamic_slice_in_dim(value_sum, start, block_rows + reach, 1) + value_acc.reshape(flat), start, 1)
        query_out = query_acc.astype(jnp.bfloat16).reshape(seq_count, block_rows, row_width)
        return (key_sum, value_sum, bias_sum + bias_terms), query_out

    init = (jnp.zeros((seq_count, length + reach, row_width), jnp.float32),
            jnp.zeros((seq_count, length + reach, row_width), jnp.float32),
            jnp.zeros((head_count, SEG, BAND), jnp.float32))
    (key_sum, value_sum, bias_sum), query_blocks = lax.scan(step, init, jnp.arange(length // block_rows, dtype=jnp.int32))
    query_grad = jnp.transpose(query_blocks, (1, 0, 2, 3)).reshape(seq_count, length, row_width)
    key_grad = key_sum[:, reach:].astype(jnp.bfloat16)
    value_grad = value_sum[:, reach:].astype(jnp.bfloat16)
    bias_grad = jax.ops.segment_sum(bias_sum.reshape(head_count, -1).T, rel_ids.reshape(-1), num_segments=BUCKETS).T
    return query_grad, key_grad, value_grad, bias_grad
```

```python
import functools

import jax
import jax.numpy as jnp
from jax import lax
from jax.experimental import pallas as pl
from jax.experimental.pallas import tpu as pltpu
from jax.sharding import PartitionSpec as P

HEAD_DIM = 128
SEG = 64
LEFT = 4
BUCKETS = 192
HALO = LEFT * SEG
PAIR = 2 * SEG
SPAN = 3 * PAIR
NEG = -1e30
LOG2E = 1.4426950408889634
MESH = pl.DeviceIdType.MESH
F32 = jnp.float32
BF16 = jnp.bfloat16
RING = 8


def dot(a, b, contract):
    return lax.dot_general(a, b, (contract, ((), ())), preferred_element_type=F32)


def lanes_of(head):
    return slice(head * HEAD_DIM, (head + 1) * HEAD_DIM)


def diagonal_sums(block):
    x = jnp.concatenate([block, jnp.zeros_like(block)], axis=1)
    rows = x.shape[0]
    while rows > 1:
        rows //= 2
        x = x[:rows] + pltpu.roll(x[rows:], 2 * PAIR - rows, 1)
    return x


def body(
    tokens, heads, q_hbm, k_hbm, v_hbm, rb_ref, g_hbm,
    dq_ref, dk_ref, dv_ref, db_ref,
    q, g, kb, vb, pt, st, tab, acc, rbs,
    out_k, out_v, in_k, in_v, by, bz, bt,
    load_sem, halo_send, halo_recv, back_send, back_recv,
    y_send, y_recv, z_send, z_recv, t_send, t_recv,
):
    sp = lax.axis_index("sp")
    tp = lax.axis_index("tp")
    ring = lax.axis_size("sp")
    tps = lax.axis_size("tp")
    zs = ring // RING
    yi = lax.rem(sp, RING)
    zi = lax.div(sp, RING)
    nxt = lax.rem(sp + 1, ring)
    prv = lax.rem(sp + ring - 1, ring)
    pairs = tokens // PAIR

    tail = tokens - HALO
    loads = []

    def load(src, dst):
        cp = pltpu.make_async_copy(src, dst, load_sem.at[len(loads)])
        cp.start()
        loads.append(cp)
        return cp

    k_tail = load(k_hbm.at[0, pl.ds(tail, HALO)], kb.at[pl.ds(HALO + tail, HALO)])
    v_tail = load(v_hbm.at[0, pl.ds(tail, HALO)], vb.at[pl.ds(HALO + tail, HALO)])
    k_head = load(k_hbm.at[0, pl.ds(0, tail)], kb.at[pl.ds(HALO, tail)])
    v_head = load(v_hbm.at[0, pl.ds(0, tail)], vb.at[pl.ds(HALO, tail)])
    q_all = load(q_hbm.at[0], q)
    g_all = load(g_hbm.at[0], g)

    y_peers = [zi * RING + lax.rem(yi + i, RING) for i in range(1, RING)]
    z_peers = [lax.rem(zi + i, zs) * RING + yi for i in range(1, zs)]
    t_peers = [lax.rem(tp + i, tps) for i in range(1, tps)]
    barrier = pltpu.get_barrier_semaphore()
    for peer in [nxt, prv] + y_peers + z_peers:
        pl.semaphore_signal(barrier, inc=1, device_id={"sp": peer}, device_id_type=MESH)
    for peer in t_peers:
        pl.semaphore_signal(barrier, inc=1, device_id={"tp": peer}, device_id_type=MESH)
    pl.semaphore_wait(barrier, 2 + len(y_peers) + len(z_peers) + len(t_peers))

    sent = []

    def send(src, dst, ssem, rsem, where):
        cp = pltpu.make_async_remote_copy(
            src_ref=src, dst_ref=dst, send_sem=ssem, recv_sem=rsem,
            device_id=where, device_id_type=MESH,
        )
        cp.start()
        sent.append(cp)
        return cp

    k_tail.wait()
    v_tail.wait()
    halo = {}
    for h in range(heads):
        for part in (1, 0):
            for a, band in enumerate((kb, vb)):
                n = len(halo)
                halo[h, a, part] = send(
                    band.at[pl.ds(tokens + part * PAIR, PAIR), pl.ds(h * HEAD_DIM, HEAD_DIM)],
                    band.at[pl.ds(part * PAIR, PAIR), pl.ds(h * HEAD_DIM, HEAD_DIM)],
                    halo_send.at[n], halo_recv.at[n], {"sp": nxt},
                )

    scale = HEAD_DIM ** (-0.5)
    neg = jnp.where(sp == 0, F32(NEG), F32(0.0))
    rbs[...] = jnp.zeros_like(rbs)
    rbs[0:heads, 0:BUCKETS] = rb_ref[...] * LOG2E
    lane = lax.broadcasted_iota(jnp.int32, (1, 2 * PAIR), 1)
    key_row = lax.broadcasted_iota(jnp.int32, (PAIR, PAIR), 0)
    q_col = lax.broadcasted_iota(jnp.int32, (PAIR, PAIR), 1)
    for h in range(heads):
        row = rbs[h : h + 1, :]
        last = rbs[h : h + 1, BUCKETS - 1 : BUCKETS]
        near = jnp.where(lane < BUCKETS, row, last)
        far = jnp.where((lane >= SEG) & (lane < BUCKETS), row, last)
        shape = (PAIR, 2 * PAIR)
        near = pltpu.roll(jnp.broadcast_to(near, shape), 193, 1, stride=1, stride_axis=0)[:, :PAIR]
        far = pltpu.roll(jnp.broadcast_to(far, shape), 65, 1, stride=1, stride_axis=0)[:, :PAIR]
        tab[h, 0:PAIR] = jnp.where((key_row < SEG) & (q_col >= SEG), NEG, last)
        tab[h, PAIR : 2 * PAIR] = far
        tab[h, 2 * PAIR : SPAN] = jnp.where((key_row >= SEG) & (q_col < SEG), NEG, near)

    for cp in (k_head, v_head, q_all, g_all):
        cp.wait()

    def block(h, p, first):
        ls = lanes_of(h)
        rows = slice(p * PAIR, p * PAIR + SPAN)
        cols = slice(p * PAIR, (p + 1) * PAIR)
        score = dot(kb[rows, ls], q[cols, ls], ((1,), (1,))) * (scale * LOG2E) + tab[h]
        outside = max(0, HALO - p * PAIR)
        if outside:
            score = jnp.concatenate([score[:outside] + neg, score[outside:]], axis=0)
        top = jnp.max(score, axis=0, keepdims=True)
        expo = jnp.exp2(score - top)
        prob = expo / jnp.sum(expo, axis=0, keepdims=True)
        pgrad = dot(vb[rows, ls], g[cols, ls], ((1,), (1,)))
        delta = jnp.sum(prob * pgrad, axis=0, keepdims=True)
        sgrad = prob * (pgrad - delta)
        pt[h, rows, cols] = prob.astype(BF16)
        st[h, rows, cols] = (sgrad * scale).astype(BF16)
        if first:
            acc[h] = sgrad
        else:
            acc[h] += sgrad

    def key_side(h, kblock, terms, other):
        p0, p1 = max(0, kblock - 2), min(pairs - 1, kblock)
        span = slice(p0 * PAIR, (p1 + 1) * PAIR)
        rows = slice(kblock * PAIR, (kblock + 1) * PAIR)
        return dot(terms[h, rows, span], other[span, lanes_of(h)], ((1,), (0,)))

    def bias_row(h):
        total = jnp.sum(acc[h, 0:PAIR], axis=0, keepdims=True)
        far = pltpu.roll(diagonal_sums(acc[h, PAIR : 2 * PAIR]), 191, 1)
        near = pltpu.roll(diagonal_sums(acc[h, 2 * PAIR : SPAN]), 63, 1)
        inner = (lane >= SEG) & (lane < BUCKETS)
        rest = jnp.where(inner, 0.0, far) + jnp.concatenate([total, jnp.zeros_like(total)], axis=1)
        rest = jnp.sum(rest, axis=1, keepdims=True)
        out = jnp.where(lane < BUCKETS, near, 0.0) + jnp.where(inner, far, 0.0)
        return out + jnp.where(lane == BUCKETS - 1, rest, 0.0)

    def give_back(h):
        ls = lanes_of(h)
        for kblock in range(HALO // PAIR):
            rows = slice(kblock * PAIR, (kblock + 1) * PAIR)
            out_k[rows, ls] = key_side(h, kblock, st, q).astype(BF16)
            out_v[rows, ls] = key_side(h, kblock, pt, g).astype(BF16)
        lane_ds = pl.ds(h * HEAD_DIM, HEAD_DIM)
        return [
            send(o.at[:, lane_ds], i.at[:, lane_ds], back_send.at[2 * h + n], back_recv.at[2 * h + n], {"sp": prv})
            for n, (o, i) in enumerate(((out_k, in_k), (out_v, in_v)))
        ]

    for h in range(heads):
        block(h, pairs - 1, True)
    back = []
    for h in range(heads):
        for p in range(pairs - 2, -1, -1):
            for a in range(2):
                halo[h, a, p].wait_recv()
            block(h, p, False)
        row = bias_row(h)
        by[yi, 2 * h : 2 * h + 1, :] = row[:, :PAIR]
        by[yi, 2 * h + 1 : 2 * h + 2, :] = row[:, PAIR:]
        if h < heads - 1:
            back += give_back(h)

    rows = 2 * heads

    def spread(buf, me, peers, axis, ssem, rsem):
        for i, peer in enumerate(peers):
            send(buf.at[me, pl.ds(0, rows)], buf.at[me, pl.ds(0, rows)], ssem.at[i], rsem.at[me], {axis: peer})

    def gathered(buf, me, count, axis, ssem, rsem):
        for i in range(1, count):
            slot = lax.rem(me + i, count)
            pltpu.make_async_remote_copy(
                src_ref=buf.at[slot, pl.ds(0, rows)], dst_ref=buf.at[slot, pl.ds(0, rows)],
                send_sem=ssem.at[0], recv_sem=rsem.at[slot],
                device_id={axis: 0}, device_id_type=MESH,
            ).wait_recv()

    spread(by, yi, y_peers, "sp", y_send, y_recv)
    back += give_back(heads - 1)

    own = tokens // PAIR
    late = HALO // PAIR
    for h in range(heads):
        ls = lanes_of(h)
        for p in range(pairs):
            rows_p = slice(p * PAIR, p * PAIR + SPAN)
            cols = slice(p * PAIR, (p + 1) * PAIR)
            dq_ref[0, cols, ls] = dot(st[h, rows_p, cols], kb[rows_p, ls], ((0,), (0,))).astype(BF16)
        for n in range(own - late):
            rows_n = slice(n * PAIR, (n + 1) * PAIR)
            dk_ref[0, rows_n, ls] = key_side(h, late + n, st, q).astype(BF16)
            dv_ref[0, rows_n, ls] = key_side(h, late + n, pt, g).astype(BF16)

    gathered(by, yi, RING, "sp", y_send, y_recv)
    total = by[0, 0:rows]
    for i in range(1, RING):
        total += by[i, 0:rows]
    bz[zi, 0:rows] = total
    spread(bz, zi, z_peers, "sp", z_send, z_recv)

    for h in range(heads):
        ls = lanes_of(h)
        for cp in back[2 * h : 2 * h + 2]:
            cp.wait_recv()
        for n in range(own - late, own):
            rows_n = slice(n * PAIR, (n + 1) * PAIR)
            rows_i = slice((n - own + late) * PAIR, (n - own + late + 1) * PAIR)
            dk_ref[0, rows_n, ls] = (key_side(h, late + n, st, q) + in_k[rows_i, ls].astype(F32)).astype(BF16)
            dv_ref[0, rows_n, ls] = (key_side(h, late + n, pt, g) + in_v[rows_i, ls].astype(F32)).astype(BF16)

    gathered(bz, zi, zs, "sp", z_send, z_recv)
    total = bz[0, 0:rows]
    for i in range(1, zs):
        total += bz[i, 0:rows]
    bt[tp, 0:rows] = total
    spread(bt, tp, t_peers, "tp", t_send, t_recv)
    gathered(bt, tp, tps, "tp", t_send, t_recv)
    for t in range(tps):
        for h in range(heads):
            r = t * heads + h
            db_ref[r : r + 1, :PAIR] = bt[t, 2 * h : 2 * h + 1, :]
            db_ref[r : r + 1, PAIR:] = bt[t, 2 * h + 1 : 2 * h + 2, : BUCKETS - PAIR]
    for cp in sent:
        cp.wait_send()


def local(queries, keys, values, rel_bias, out_grad):
    _, tokens, width = queries.shape
    heads = width // HEAD_DIM
    tps = lax.axis_size("tp")
    zs = lax.axis_size("sp") // RING
    band = tokens + HALO
    dma = pltpu.SemaphoreType.DMA
    grad = jax.ShapeDtypeStruct(queries.shape, BF16)
    anywhere = pl.BlockSpec(memory_space=pl.ANY)
    vmem = pl.BlockSpec(memory_space=pltpu.VMEM)
    return pl.pallas_call(
        functools.partial(body, tokens, heads),
        out_shape=(grad, grad, grad, jax.ShapeDtypeStruct((heads * tps, BUCKETS), F32)),
        in_specs=[anywhere, anywhere, anywhere, vmem, anywhere],
        out_specs=(vmem, vmem, vmem, vmem),
        scratch_shapes=[
            pltpu.VMEM((tokens, width), BF16),
            pltpu.VMEM((tokens, width), BF16),
            pltpu.VMEM((band, width), BF16),
            pltpu.VMEM((band, width), BF16),
            pltpu.VMEM((heads, band, tokens), BF16),
            pltpu.VMEM((heads, band, tokens), BF16),
            pltpu.VMEM((heads, SPAN, PAIR), F32),
            pltpu.VMEM((heads, SPAN, PAIR), F32),
            pltpu.VMEM((8, 2 * PAIR), F32),
            pltpu.VMEM((HALO, width), BF16),
            pltpu.VMEM((HALO, width), BF16),
            pltpu.VMEM((HALO, width), BF16),
            pltpu.VMEM((HALO, width), BF16),
            pltpu.VMEM((RING, 8, PAIR), F32),
            pltpu.VMEM((zs, 8, PAIR), F32),
            pltpu.VMEM((tps, 8, PAIR), F32),
            dma((6,)),
            dma((4 * heads,)),
            dma((4 * heads,)),
            dma((2 * heads,)),
            dma((2 * heads,)),
            dma((RING,)),
            dma((RING,)),
            dma((zs,)),
            dma((zs,)),
            dma((tps,)),
            dma((tps,)),
        ],
        compiler_params=pltpu.CompilerParams(collective_id=0, has_side_effects=True),
    )(queries, keys, values, rel_bias, out_grad)


def solution(mesh):
    return jax.shard_map(
        local,
        mesh=mesh,
        in_specs=(
            P(None, "sp", "tp"),
            P(None, "sp", "tp"),
            P(None, "sp", "tp"),
            P("tp", None),
            P(None, "sp", "tp"),
        ),
        out_specs=(P(None, "sp", "tp"), P(None, "sp", "tp"), P(None, "sp", "tp"), P()),
        check_vma=False,
    )
```

```python
import functools

import jax
import jax.numpy as jnp
from jax import lax
from jax.experimental import pallas as pl
from jax.experimental.pallas import tpu as pltpu
from jax.sharding import PartitionSpec as P

HEAD_DIM = 128
SEG = 64
LEFT = 4
BUCKETS = 192
HALO = LEFT * SEG
PAIR = 2 * SEG
SPAN = 3 * PAIR
NEG = -1e30
LOG2E = 1.4426950408889634
MESH = pl.DeviceIdType.MESH
F32 = jnp.float32
BF16 = jnp.bfloat16
RING = 8


def dot(a, b, contract):
    return lax.dot_general(a, b, (contract, ((), ())), preferred_element_type=F32)


def lanes_of(head):
    return slice(head * HEAD_DIM, (head + 1) * HEAD_DIM)


def diagonal_sums(block):
    x = jnp.concatenate([block, jnp.zeros_like(block)], axis=1)
    rows = x.shape[0]
    while rows > 1:
        rows //= 2
        x = x[:rows] + pltpu.roll(x[rows:], 2 * PAIR - rows, 1)
    return x


def body(
    tokens, heads, q_hbm, k_hbm, v_hbm, rb_ref, g_hbm,
    dq_ref, dk_ref, dv_ref, db_ref,
    q, g, kb, vb, pt, st, tab, acc, rbs,
    out_k, out_v, in_k, in_v, by, bz, bt,
    load_sem, halo_send, halo_recv, back_send, back_recv,
    y_send, y_recv, z_send, z_recv, t_send, t_recv,
):
    sp = lax.axis_index("sp")
    tp = lax.axis_index("tp")
    ring = lax.axis_size("sp")
    tps = lax.axis_size("tp")
    zs = ring // RING
    yi = lax.rem(sp, RING)
    zi = lax.div(sp, RING)
    nxt = lax.rem(sp + 1, ring)
    prv = lax.rem(sp + ring - 1, ring)
    pairs = tokens // PAIR

    tail = tokens - HALO
    loads = []

    def load(src, dst):
        cp = pltpu.make_async_copy(src, dst, load_sem.at[len(loads)])
        cp.start()
        loads.append(cp)
        return cp

    k_tail = load(k_hbm.at[0, pl.ds(tail, HALO)], kb.at[pl.ds(HALO + tail, HALO)])
    v_tail = load(v_hbm.at[0, pl.ds(tail, HALO)], vb.at[pl.ds(HALO + tail, HALO)])
    k_head = load(k_hbm.at[0, pl.ds(0, tail)], kb.at[pl.ds(HALO, tail)])
    v_head = load(v_hbm.at[0, pl.ds(0, tail)], vb.at[pl.ds(HALO, tail)])
    q_all = load(q_hbm.at[0], q)
    g_all = load(g_hbm.at[0], g)

    y_peers = [zi * RING + lax.rem(yi + i, RING) for i in range(1, RING)]
    z_peers = [lax.rem(zi + i, zs) * RING + yi for i in range(1, zs)]
    t_peers = [lax.rem(tp + i, tps) for i in range(1, tps)]
    barrier = pltpu.get_barrier_semaphore()
    for peer in [nxt, prv] + y_peers + z_peers:
        pl.semaphore_signal(barrier, inc=1, device_id={"sp": peer}, device_id_type=MESH)
    for peer in t_peers:
        pl.semaphore_signal(barrier, inc=1, device_id={"tp": peer}, device_id_type=MESH)
    pl.semaphore_wait(barrier, 2 + len(y_peers) + len(z_peers) + len(t_peers))

    sent = []

    def send(src, dst, ssem, rsem, where):
        cp = pltpu.make_async_remote_copy(
            src_ref=src, dst_ref=dst, send_sem=ssem, recv_sem=rsem,
            device_id=where, device_id_type=MESH,
        )
        cp.start()
        sent.append(cp)
        return cp

    k_tail.wait()
    v_tail.wait()
    halo = {}
    for h in range(heads):
        for part in (1, 0):
            for a, band in enumerate((kb, vb)):
                n = len(halo)
                halo[h, a, part] = send(
                    band.at[pl.ds(tokens + part * PAIR, PAIR), pl.ds(h * HEAD_DIM, HEAD_DIM)],
                    band.at[pl.ds(part * PAIR, PAIR), pl.ds(h * HEAD_DIM, HEAD_DIM)],
                    halo_send.at[n], halo_recv.at[n], {"sp": nxt},
                )

    scale = HEAD_DIM ** (-0.5)
    neg = jnp.where(sp == 0, F32(NEG), F32(0.0))
    rbs[...] = jnp.zeros_like(rbs)
    rbs[0:heads, 0:BUCKETS] = rb_ref[...] * LOG2E
    lane = lax.broadcasted_iota(jnp.int32, (1, 2 * PAIR), 1)
    key_row = lax.broadcasted_iota(jnp.int32, (PAIR, PAIR), 0)
    q_col = lax.broadcasted_iota(jnp.int32, (PAIR, PAIR), 1)
    for h in range(heads):
        row = rbs[h : h + 1, :]
        last = rbs[h : h + 1, BUCKETS - 1 : BUCKETS]
        near = jnp.where(lane < BUCKETS, row, last)
        far = jnp.where((lane >= SEG) & (lane < BUCKETS), row, last)
        shape = (PAIR, 2 * PAIR)
        near = pltpu.roll(jnp.broadcast_to(near, shape), 193, 1, stride=1, stride_axis=0)[:, :PAIR]
        far = pltpu.roll(jnp.broadcast_to(far, shape), 65, 1, stride=1, stride_axis=0)[:, :PAIR]
        tab[h, 0:PAIR] = jnp.where((key_row < SEG) & (q_col >= SEG), NEG, last)
        tab[h, PAIR : 2 * PAIR] = far
        tab[h, 2 * PAIR : SPAN] = jnp.where((key_row >= SEG) & (q_col < SEG), NEG, near)

    for cp in (k_head, v_head, q_all, g_all):
        cp.wait()

    def block(h, p, first):
        ls = lanes_of(h)
        rows = slice(p * PAIR, p * PAIR + SPAN)
        cols = slice(p * PAIR, (p + 1) * PAIR)
        score = dot(kb[rows, ls], q[cols, ls], ((1,), (1,))) * (scale * LOG2E) + tab[h]
        outside = max(0, HALO - p * PAIR)
        if outside:
            score = jnp.concatenate([score[:outside] + neg, score[outside:]], axis=0)
        top = jnp.max(score, axis=0, keepdims=True)
        expo = jnp.exp2(score - top)
        prob = expo / jnp.sum(expo, axis=0, keepdims=True)
        pgrad = dot(vb[rows, ls], g[cols, ls], ((1,), (1,)))
        delta = jnp.sum(prob * pgrad, axis=0, keepdims=True)
        sgrad = prob * (pgrad - delta)
        pt[h, rows, cols] = prob.astype(BF16)
        st[h, rows, cols] = (sgrad * scale).astype(BF16)
        if first:
            acc[h] = sgrad
        else:
            acc[h] += sgrad

    def key_side(h, kblock, terms, other):
        p0, p1 = max(0, kblock - 2), min(pairs - 1, kblock)
        span = slice(p0 * PAIR, (p1 + 1) * PAIR)
        rows = slice(kblock * PAIR, (kblock + 1) * PAIR)
        return dot(terms[h, rows, span], other[span, lanes_of(h)], ((1,), (0,)))

    def bias_row(h):
        total = jnp.sum(acc[h, 0:PAIR], axis=0, keepdims=True)
        far = pltpu.roll(diagonal_sums(acc[h, PAIR : 2 * PAIR]), 191, 1)
        near = pltpu.roll(diagonal_sums(acc[h, 2 * PAIR : SPAN]), 63, 1)
        inner = (lane >= SEG) & (lane < BUCKETS)
        rest = jnp.where(inner, 0.0, far) + jnp.concatenate([total, jnp.zeros_like(total)], axis=1)
        rest = jnp.sum(rest, axis=1, keepdims=True)
        out = jnp.where(lane < BUCKETS, near, 0.0) + jnp.where(inner, far, 0.0)
        return out + jnp.where(lane == BUCKETS - 1, rest, 0.0)

    def give_back(h):
        ls = lanes_of(h)
        for kblock in range(HALO // PAIR):
            rows = slice(kblock * PAIR, (kblock + 1) * PAIR)
            out_k[rows, ls] = key_side(h, kblock, st, q).astype(BF16)
            out_v[rows, ls] = key_side(h, kblock, pt, g).astype(BF16)
        lane_ds = pl.ds(h * HEAD_DIM, HEAD_DIM)
        return [
            send(o.at[:, lane_ds], i.at[:, lane_ds], back_send.at[2 * h + n], back_recv.at[2 * h + n], {"sp": prv})
            for n, (o, i) in enumerate(((out_k, in_k), (out_v, in_v)))
        ]

    for h in range(heads):
        block(h, pairs - 1, True)
    back = []
    for h in range(heads):
        for p in range(pairs - 2, -1, -1):
            for a in range(2):
                halo[h, a, p].wait_recv()
            block(h, p, False)
        row = bias_row(h)
        by[yi, 2 * h : 2 * h + 1, :] = row[:, :PAIR]
        by[yi, 2 * h + 1 : 2 * h + 2, :] = row[:, PAIR:]
        if h < heads - 1:
            back += give_back(h)

    rows = 2 * heads

    def spread(buf, me, peers, axis, ssem, rsem):
        for i, peer in enumerate(peers):
            send(buf.at[me, pl.ds(0, rows)], buf.at[me, pl.ds(0, rows)], ssem.at[i], rsem.at[me], {axis: peer})

    def gathered(buf, me, count, axis, ssem, rsem):
        for i in range(1, count):
            slot = lax.rem(me + i, count)
            pltpu.make_async_remote_copy(
                src_ref=buf.at[slot, pl.ds(0, rows)], dst_ref=buf.at[slot, pl.ds(0, rows)],
                send_sem=ssem.at[0], recv_sem=rsem.at[slot],
                device_id={axis: 0}, device_id_type=MESH,
            ).wait_recv()

    spread(by, yi, y_peers, "sp", y_send, y_recv)
    back += give_back(heads - 1)

    own = tokens // PAIR
    late = HALO // PAIR
    for h in range(heads):
        ls = lanes_of(h)
        for p in range(pairs):
            rows_p = slice(p * PAIR, p * PAIR + SPAN)
            cols = slice(p * PAIR, (p + 1) * PAIR)
            dq_ref[0, cols, ls] = dot(st[h, rows_p, cols], kb[rows_p, ls], ((0,), (0,))).astype(BF16)
        for n in range(own - late):
            rows_n = slice(n * PAIR, (n + 1) * PAIR)
            dk_ref[0, rows_n, ls] = key_side(h, late + n, st, q).astype(BF16)
            dv_ref[0, rows_n, ls] = key_side(h, late + n, pt, g).astype(BF16)

    gathered(by, yi, RING, "sp", y_send, y_recv)
    total = by[0, 0:rows]
    for i in range(1, RING):
        total += by[i, 0:rows]
    bz[zi, 0:rows] = total
    spread(bz, zi, z_peers, "sp", z_send, z_recv)

    for h in range(heads):
        ls = lanes_of(h)
        for cp in back[2 * h : 2 * h + 2]:
            cp.wait_recv()
        for n in range(own - late, own):
            rows_n = slice(n * PAIR, (n + 1) * PAIR)
            rows_i = slice((n - own + late) * PAIR, (n - own + late + 1) * PAIR)
            dk_ref[0, rows_n, ls] = (key_side(h, late + n, st, q) + in_k[rows_i, ls].astype(F32)).astype(BF16)
            dv_ref[0, rows_n, ls] = (key_side(h, late + n, pt, g) + in_v[rows_i, ls].astype(F32)).astype(BF16)

    gathered(bz, zi, zs, "sp", z_send, z_recv)
    total = bz[0, 0:rows]
    for i in range(1, zs):
        total += bz[i, 0:rows]
    bt[tp, 0:rows] = total
    spread(bt, tp, t_peers, "tp", t_send, t_recv)
    gathered(bt, tp, tps, "tp", t_send, t_recv)
    for t in range(tps):
        for h in range(heads):
            r = t * heads + h
            db_ref[r : r + 1, :PAIR] = bt[t, 2 * h : 2 * h + 1, :]
            db_ref[r : r + 1, PAIR:] = bt[t, 2 * h + 1 : 2 * h + 2, : BUCKETS - PAIR]
    for cp in sent:
        cp.wait_send()


def put_out(*refs):
    ins, outs, sem = refs[:4], refs[4:8], refs[8]
    copies = [pltpu.make_async_copy(i, o, sem.at[n]) for n, (i, o) in enumerate(zip(ins, outs))]
    for cp in copies:
        cp.start()
    for cp in copies:
        cp.wait()


def local(queries, keys, values, rel_bias, out_grad):
    _, tokens, width = queries.shape
    heads = width // HEAD_DIM
    tps = lax.axis_size("tp")
    zs = lax.axis_size("sp") // RING
    band = tokens + HALO
    dma = pltpu.SemaphoreType.DMA
    grad = jax.ShapeDtypeStruct(queries.shape, BF16)
    anywhere = pl.BlockSpec(memory_space=pl.ANY)
    vmem = pl.BlockSpec(memory_space=pltpu.VMEM)
    bias = jax.ShapeDtypeStruct((heads * tps, BUCKETS), F32)
    outs = (grad, grad, grad, bias)
    held = pl.pallas_call(
        functools.partial(body, tokens, heads),
        out_shape=tuple(pltpu.VMEM(o.shape, o.dtype) for o in outs),
        in_specs=[anywhere, anywhere, anywhere, vmem, anywhere],
        out_specs=(vmem, vmem, vmem, vmem),
        scratch_shapes=[
            pltpu.VMEM((tokens, width), BF16),
            pltpu.VMEM((tokens, width), BF16),
            pltpu.VMEM((band, width), BF16),
            pltpu.VMEM((band, width), BF16),
            pltpu.VMEM((heads, band, tokens), BF16),
            pltpu.VMEM((heads, band, tokens), BF16),
            pltpu.VMEM((heads, SPAN, PAIR), F32),
            pltpu.VMEM((heads, SPAN, PAIR), F32),
            pltpu.VMEM((8, 2 * PAIR), F32),
            pltpu.VMEM((HALO, width), BF16),
            pltpu.VMEM((HALO, width), BF16),
            pltpu.VMEM((HALO, width), BF16),
            pltpu.VMEM((HALO, width), BF16),
            pltpu.VMEM((RING, 8, PAIR), F32),
            pltpu.VMEM((zs, 8, PAIR), F32),
            pltpu.VMEM((tps, 8, PAIR), F32),
            dma((6,)),
            dma((4 * heads,)),
            dma((4 * heads,)),
            dma((2 * heads,)),
            dma((2 * heads,)),
            dma((RING,)),
            dma((RING,)),
            dma((zs,)),
            dma((zs,)),
            dma((tps,)),
            dma((tps,)),
        ],
        compiler_params=pltpu.CompilerParams(collective_id=0, has_side_effects=True),
    )(queries, keys, values, rel_bias, out_grad)
    return pl.pallas_call(
        put_out,
        out_shape=outs,
        in_specs=[vmem] * 4,
        out_specs=(anywhere,) * 4,
        scratch_shapes=[dma((4,))],
    )(*[pltpu.with_memory_space_constraint(x, pltpu.VMEM) for x in held])


def solution(mesh):
    return jax.shard_map(
        local,
        mesh=mesh,
        in_specs=(
            P(None, "sp", "tp"),
            P(None, "sp", "tp"),
            P(None, "sp", "tp"),
            P("tp", None),
            P(None, "sp", "tp"),
        ),
        out_specs=(P(None, "sp", "tp"), P(None, "sp", "tp"), P(None, "sp", "tp"), P()),
        check_vma=False,
    )
```

```python
import functools
import itertools

import jax
import jax.numpy as jnp
from jax import lax
from jax.experimental import pallas as pl
from jax.experimental.pallas import tpu as pltpu
from jax.sharding import PartitionSpec as P

HEAD_DIM = 128
SEG = 64
LEFT = 4
BUCKETS = 192
HALO = LEFT * SEG
PAIR = 2 * SEG
SPAN = 3 * PAIR
NEG = -1e30
LOG2E = 1.4426950408889634
MESH = pl.DeviceIdType.MESH
F32 = jnp.float32
BF16 = jnp.bfloat16
RING = 8


def dot(a, b, contract):
    return lax.dot_general(a, b, (contract, ((), ())), preferred_element_type=F32)


def lanes_of(head):
    return slice(head * HEAD_DIM, (head + 1) * HEAD_DIM)


def diagonal_sums(block, offset):
    x = jnp.concatenate([block, jnp.zeros_like(block)], axis=1)
    span = 2 * PAIR
    eight = jnp.zeros((8, span), F32)
    for r in range(0, x.shape[0], 8):
        eight += pltpu.roll(x[r : r + 8], (offset - r) % span, 1)
    row = lax.broadcasted_iota(jnp.int32, (8, span), 0)
    out = jnp.where(row == 0, eight, 0.0)
    for r in range(1, 8):
        out += jnp.where(row == r, pltpu.roll(eight, span - r, 1), 0.0)
    return jnp.sum(out, axis=0, keepdims=True)


def body(
    tokens, heads, q_hbm, k_hbm, v_hbm, rb_ref, g_hbm,
    dq_ref, dk_ref, dv_ref, db_ref,
    q, g, kb, vb, pt, st, tab, acc, rbs,
    out_k, out_v, in_k, in_v, by, bz, round_sem,
    load_sem, halo_send, halo_recv, back_send, back_recv,
    y_send, y_recv, z_send, z_recv,
):
    sp = lax.axis_index("sp")
    tp = lax.axis_index("tp")
    ring = lax.axis_size("sp")
    tps = lax.axis_size("tp")
    zs = ring // RING
    yi = lax.rem(sp, RING)
    zi = lax.div(sp, RING)
    nxt = lax.rem(sp + 1, ring)
    prv = lax.rem(sp + ring - 1, ring)
    pairs = tokens // PAIR

    tail = tokens - HALO
    loads = []

    def load(src, dst):
        cp = pltpu.make_async_copy(src, dst, load_sem.at[len(loads)])
        cp.start()
        loads.append(cp)
        return cp

    k_tail = load(k_hbm.at[0, pl.ds(tail, HALO)], kb.at[pl.ds(HALO + tail, HALO)])
    v_tail = load(v_hbm.at[0, pl.ds(tail, HALO)], vb.at[pl.ds(HALO + tail, HALO)])
    k_head = load(k_hbm.at[0, pl.ds(0, tail)], kb.at[pl.ds(HALO, tail)])
    v_head = load(v_hbm.at[0, pl.ds(0, tail)], vb.at[pl.ds(HALO, tail)])
    q_all = load(q_hbm.at[0], q)
    g_all = load(g_hbm.at[0], g)

    sizes = {"z": zs, "y": RING, "x": tps // 2, "c": 2}
    here = {"z": zi, "y": yi, "x": lax.div(tp, 2), "c": lax.rem(tp, 2)}

    def at(**moves):
        c = {a: lax.rem(here[a] + moves[a], sizes[a]) if a in moves else here[a] for a in sizes}
        return {"sp": c["z"] * RING + c["y"], "tp": c["x"] * 2 + c["c"]}

    def steps(reach, axes):
        return [(a, m) for a in axes for m in sorted({r % sizes[a] for r in reach} - {0})]

    def greet(sem, moves, extra=()):
        for where in [at(**{a: m}) for a, m in moves] + list(extra):
            pl.semaphore_signal(sem, inc=1, device_id=where, device_id_type=MESH)
        return len(moves) + len(extra)

    def hear(sem, count):
        if count:
            pl.semaphore_wait(sem, count)

    near = steps((1, -1), "zyxc")
    barrier = pltpu.get_barrier_semaphore()
    pl.semaphore_wait(barrier, greet(barrier, near, [{"sp": nxt}, {"sp": prv}]))

    sent = []

    def send(src, dst, ssem, rsem, where):
        cp = pltpu.make_async_remote_copy(
            src_ref=src, dst_ref=dst, send_sem=ssem, recv_sem=rsem,
            device_id=where, device_id_type=MESH,
        )
        cp.start()
        sent.append(cp)
        return cp

    k_tail.wait()
    v_tail.wait()
    halo = {}
    for h in range(heads):
        for part in (1, 0):
            for a, band in enumerate((kb, vb)):
                n = len(halo)
                halo[h, a, part] = send(
                    band.at[pl.ds(tokens + part * PAIR, PAIR), pl.ds(h * HEAD_DIM, HEAD_DIM)],
                    band.at[pl.ds(part * PAIR, PAIR), pl.ds(h * HEAD_DIM, HEAD_DIM)],
                    halo_send.at[n], halo_recv.at[n], {"sp": nxt},
                )

    heard = greet(round_sem.at[0], near)

    scale = HEAD_DIM ** (-0.5)
    neg = jnp.where(sp == 0, F32(NEG), F32(0.0))
    rbs[...] = jnp.zeros_like(rbs)
    rbs[0:heads, 0:BUCKETS] = rb_ref[...] * LOG2E
    lane = lax.broadcasted_iota(jnp.int32, (1, 2 * PAIR), 1)
    key_row = lax.broadcasted_iota(jnp.int32, (PAIR, PAIR), 0)
    q_col = lax.broadcasted_iota(jnp.int32, (PAIR, PAIR), 1)
    for h in range(heads):
        row = rbs[h : h + 1, :]
        last = rbs[h : h + 1, BUCKETS - 1 : BUCKETS]
        near = jnp.where(lane < BUCKETS, row, last)
        far = jnp.where((lane >= SEG) & (lane < BUCKETS), row, last)
        shape = (PAIR, 2 * PAIR)
        near = pltpu.roll(jnp.broadcast_to(near, shape), 193, 1, stride=1, stride_axis=0)[:, :PAIR]
        far = pltpu.roll(jnp.broadcast_to(far, shape), 65, 1, stride=1, stride_axis=0)[:, :PAIR]
        tab[h, 0:PAIR] = jnp.where((key_row < SEG) & (q_col >= SEG), NEG, last)
        tab[h, PAIR : 2 * PAIR] = far
        tab[h, 2 * PAIR : SPAN] = jnp.where((key_row >= SEG) & (q_col < SEG), NEG, near)

    for cp in (k_head, v_head, q_all, g_all):
        cp.wait()

    def block(h, p, first):
        ls = lanes_of(h)
        rows = slice(p * PAIR, p * PAIR + SPAN)
        cols = slice(p * PAIR, (p + 1) * PAIR)
        score = dot(kb[rows, ls], q[cols, ls], ((1,), (1,))) * (scale * LOG2E) + tab[h]
        outside = max(0, HALO - p * PAIR)
        if outside:
            score = jnp.concatenate([score[:outside] + neg, score[outside:]], axis=0)
        top = jnp.max(score, axis=0, keepdims=True)
        expo = jnp.exp2(score - top)
        prob = expo / jnp.sum(expo, axis=0, keepdims=True)
        pgrad = dot(vb[rows, ls], g[cols, ls], ((1,), (1,)))
        delta = jnp.sum(prob * pgrad, axis=0, keepdims=True)
        sgrad = prob * (pgrad - delta)
        pt[h, rows, cols] = prob.astype(BF16)
        st[h, rows, cols] = (sgrad * scale).astype(BF16)
        if first:
            acc[h] = sgrad
        else:
            acc[h] += sgrad

    def key_side(h, kblock, terms, other):
        p0, p1 = max(0, kblock - 2), min(pairs - 1, kblock)
        span = slice(p0 * PAIR, (p1 + 1) * PAIR)
        rows = slice(kblock * PAIR, (kblock + 1) * PAIR)
        return dot(terms[h, rows, span], other[span, lanes_of(h)], ((1,), (0,)))

    def bias_row(h):
        base = SEG * h
        total = jnp.sum(acc[h, 0:PAIR], axis=0, keepdims=True)
        far = diagonal_sums(acc[h, PAIR : 2 * PAIR], 191 + base)
        near = diagonal_sums(acc[h, 2 * PAIR : SPAN], 63 + base)
        place = lane - base
        inner = (place >= SEG) & (place < BUCKETS)
        rest = jnp.where(inner, 0.0, far) + jnp.concatenate([total, jnp.zeros_like(total)], axis=1)
        rest = jnp.sum(rest, axis=1, keepdims=True)
        out = jnp.where((place >= 0) & (place < BUCKETS), near, 0.0) + jnp.where(inner, far, 0.0)
        return out + jnp.where(place == BUCKETS - 1, rest, 0.0)

    def give_back(h):
        ls = lanes_of(h)
        for kblock in range(HALO // PAIR):
            rows = slice(kblock * PAIR, (kblock + 1) * PAIR)
            out_k[rows, ls] = key_side(h, kblock, st, q).astype(BF16)
            out_v[rows, ls] = key_side(h, kblock, pt, g).astype(BF16)
        lane_ds = pl.ds(h * HEAD_DIM, HEAD_DIM)
        return [
            send(o.at[:, lane_ds], i.at[:, lane_ds], back_send.at[2 * h + n], back_recv.at[2 * h + n], {"sp": prv})
            for n, (o, i) in enumerate(((out_k, in_k), (out_v, in_v)))
        ]

    for h in range(heads):
        block(h, pairs - 1, True)
    hear(round_sem.at[0], heard)
    heard = greet(round_sem.at[1], steps((2, -2), "zy"))
    back = []
    rows_of = []
    for h in range(heads):
        for p in range(pairs - 2, -1, -1):
            for a in range(2):
                halo[h, a, p].wait_recv()
            block(h, p, False)
        rows_of.append(bias_row(h))
        if h == 0:
            hear(round_sem.at[1], heard)
            heard = greet(round_sem.at[2], steps((1, 2, 3), "xc"))
            back += give_back(h)
    hear(round_sem.at[2], heard)

    def spread(buf, axes, rows, ssem, rsem, values):
        moves = [m for m in itertools.product(*(range(sizes[a]) for a in axes)) if any(m)]
        moves.sort(key=lambda m: -sum(min(v, sizes[a] - v) for a, v in zip(axes, m)))

        def slot(m):
            n = 0
            for a, v in zip(axes, m):
                n = n * sizes[a] + lax.rem(here[a] + v, sizes[a])
            return n

        mine = slot((0,) * len(axes))
        for r, value in enumerate(values):
            buf[mine, r : r + 1, :] = value
        part = pl.ds(0, rows)
        for n, m in enumerate(moves):
            send(buf.at[mine, part], buf.at[mine, part], ssem.at[n], rsem.at[mine], at(**dict(zip(axes, m))))

        def collect():
            for m in reversed(moves):
                other = buf.at[slot(m), part]
                pltpu.make_async_remote_copy(
                    src_ref=other, dst_ref=other, send_sem=ssem.at[0], recv_sem=rsem.at[slot(m)],
                    device_id=at(), device_id_type=MESH,
                ).wait_recv()

        return collect

    first, second = rows_of
    collect = spread(
        bz, "zc", 3, z_send, z_recv,
        [first[:, :PAIR], first[:, PAIR:] + second[:, :PAIR], second[:, PAIR:]],
    )
    back += give_back(heads - 1)

    own = tokens // PAIR
    late = HALO // PAIR
    for h in range(heads):
        ls = lanes_of(h)
        for p in range(pairs):
            rows_p = slice(p * PAIR, p * PAIR + SPAN)
            cols = slice(p * PAIR, (p + 1) * PAIR)
            dq_ref[0, cols, ls] = dot(st[h, rows_p, cols], kb[rows_p, ls], ((0,), (0,))).astype(BF16)
        for n in range(own - late):
            rows_n = slice(n * PAIR, (n + 1) * PAIR)
            dk_ref[0, rows_n, ls] = key_side(h, late + n, st, q).astype(BF16)
            dv_ref[0, rows_n, ls] = key_side(h, late + n, pt, g).astype(BF16)

    collect()
    values = []
    for c in range(2):
        total = bz[c, 0:3]
        for z in range(1, zs):
            total += bz[2 * z + c, 0:3]
        values += [total[r : r + 1] for r in range(3)]
    collect = spread(by, "yx", 6, y_send, y_recv, values)

    for h in range(heads):
        ls = lanes_of(h)
        for cp in back[2 * h : 2 * h + 2]:
            cp.wait_recv()
        for n in range(own - late, own):
            rows_n = slice(n * PAIR, (n + 1) * PAIR)
            rows_i = slice((n - own + late) * PAIR, (n - own + late + 1) * PAIR)
            dk_ref[0, rows_n, ls] = (key_side(h, late + n, st, q) + in_k[rows_i, ls].astype(F32)).astype(BF16)
            dv_ref[0, rows_n, ls] = (key_side(h, late + n, pt, g) + in_v[rows_i, ls].astype(F32)).astype(BF16)

    collect()
    xs = tps // 2
    for x in range(xs):
        total = by[x, 0:6]
        for y in range(1, RING):
            total += by[y * xs + x, 0:6]
        for c in range(2):
            r = 2 * (2 * x + c)
            low, mid, high = (total[3 * c + n : 3 * c + n + 1] for n in range(3))
            db_ref[r : r + 1, :PAIR] = low
            db_ref[r : r + 1, PAIR:] = mid[:, : BUCKETS - PAIR]
            both = pltpu.roll(jnp.concatenate([mid, high], axis=1), 2 * PAIR - SEG, 1)
            db_ref[r + 1 : r + 2, :PAIR] = both[:, :PAIR]
            db_ref[r + 1 : r + 2, PAIR:] = both[:, PAIR:BUCKETS]
    for cp in sent:
        cp.wait_send()


def put_out(*refs):
    ins, outs, sem = refs[:4], refs[4:8], refs[8]
    copies = [pltpu.make_async_copy(i, o, sem.at[n]) for n, (i, o) in enumerate(zip(ins, outs))]
    for cp in copies:
        cp.start()
    for cp in copies:
        cp.wait()


def local(queries, keys, values, rel_bias, out_grad):
    _, tokens, width = queries.shape
    heads = width // HEAD_DIM
    tps = lax.axis_size("tp")
    zs = lax.axis_size("sp") // RING
    band = tokens + HALO
    dma = pltpu.SemaphoreType.DMA
    grad = jax.ShapeDtypeStruct(queries.shape, BF16)
    anywhere = pl.BlockSpec(memory_space=pl.ANY)
    vmem = pl.BlockSpec(memory_space=pltpu.VMEM)
    bias = jax.ShapeDtypeStruct((heads * tps, BUCKETS), F32)
    outs = (grad, grad, grad, bias)
    held = pl.pallas_call(
        functools.partial(body, tokens, heads),
        out_shape=tuple(pltpu.VMEM(o.shape, o.dtype) for o in outs),
        in_specs=[anywhere, anywhere, anywhere, vmem, anywhere],
        out_specs=(vmem, vmem, vmem, vmem),
        scratch_shapes=[
            pltpu.VMEM((tokens, width), BF16),
            pltpu.VMEM((tokens, width), BF16),
            pltpu.VMEM((band, width), BF16),
            pltpu.VMEM((band, width), BF16),
            pltpu.VMEM((heads, band, tokens), BF16),
            pltpu.VMEM((heads, band, tokens), BF16),
            pltpu.VMEM((heads, SPAN, PAIR), F32),
            pltpu.VMEM((heads, SPAN, PAIR), F32),
            pltpu.VMEM((8, 2 * PAIR), F32),
            pltpu.VMEM((HALO, width), BF16),
            pltpu.VMEM((HALO, width), BF16),
            pltpu.VMEM((HALO, width), BF16),
            pltpu.VMEM((HALO, width), BF16),
            pltpu.VMEM((RING * tps // 2, 8, PAIR), F32),
            pltpu.VMEM((zs * 2, 8, PAIR), F32),
            pltpu.SemaphoreType.REGULAR((3,)),
            dma((6,)),
            dma((4 * heads,)),
            dma((4 * heads,)),
            dma((2 * heads,)),
            dma((2 * heads,)),
            dma((RING * tps // 2,)),
            dma((RING * tps // 2,)),
            dma((zs * 2,)),
            dma((zs * 2,)),
        ],
        compiler_params=pltpu.CompilerParams(collective_id=0, has_side_effects=True),
    )(queries, keys, values, rel_bias, out_grad)
    return pl.pallas_call(
        put_out,
        out_shape=outs,
        in_specs=[vmem] * 4,
        out_specs=(anywhere,) * 4,
        scratch_shapes=[dma((4,))],
    )(*[pltpu.with_memory_space_constraint(x, pltpu.VMEM) for x in held])


def solution(mesh):
    return jax.shard_map(
        local,
        mesh=mesh,
        in_specs=(
            P(None, "sp", "tp"),
            P(None, "sp", "tp"),
            P(None, "sp", "tp"),
            P("tp", None),
            P(None, "sp", "tp"),
        ),
        out_specs=(P(None, "sp", "tp"), P(None, "sp", "tp"), P(None, "sp", "tp"), P()),
        check_vma=False,
    )
```

```python
import functools
import itertools

import jax
import jax.numpy as jnp
from jax import lax
from jax.experimental import pallas as pl
from jax.experimental.pallas import tpu as pltpu
from jax.sharding import PartitionSpec as P

HEAD_DIM = 128
SEG = 64
LEFT = 4
BUCKETS = 192
HALO = LEFT * SEG
PAIR = 2 * SEG
SPAN = 3 * PAIR
NEG = -1e30
LOG2E = 1.4426950408889634
MESH = pl.DeviceIdType.MESH
F32 = jnp.float32
BF16 = jnp.bfloat16
RING = 8


def dot(a, b, contract):
    return lax.dot_general(a, b, (contract, ((), ())), preferred_element_type=F32)


def lanes_of(head):
    return slice(head * HEAD_DIM, (head + 1) * HEAD_DIM)


def diagonal_sums(block, offset):
    x = jnp.concatenate([block, jnp.zeros_like(block)], axis=1)
    span = 2 * PAIR
    eight = jnp.zeros((8, span), F32)
    for r in range(0, x.shape[0], 8):
        eight += pltpu.roll(x[r : r + 8], (offset - r) % span, 1)
    row = lax.broadcasted_iota(jnp.int32, (8, span), 0)
    out = jnp.where(row == 0, eight, 0.0)
    for r in range(1, 8):
        out += jnp.where(row == r, pltpu.roll(eight, span - r, 1), 0.0)
    return jnp.sum(out, axis=0, keepdims=True)


def body(
    tokens, heads, q_hbm, k_hbm, v_hbm, rb_hbm, g_hbm,
    dq_ref, dk_ref, dv_ref, db_ref,
    q, g, q0, g0, kb, vb, pt, st, tab, acc, rbs, rb,
    out_k, out_v, in_k, in_v, fwd, got, part_k, part_v, by, bz, round_sem,
    load_sem, halo_send, halo_recv, ahead_send, ahead_recv,
    back_send, back_recv, fwd_send, fwd_recv,
    y_send, y_recv, z_send, z_recv,
):
    sp = lax.axis_index("sp")
    tp = lax.axis_index("tp")
    ring = lax.axis_size("sp")
    tps = lax.axis_size("tp")
    zs = ring // RING
    yi = lax.rem(sp, RING)
    zi = lax.div(sp, RING)
    nxt = lax.rem(sp + 1, ring)
    prv = lax.rem(sp + ring - 1, ring)
    pairs = tokens // PAIR

    sizes = {"z": zs, "y": RING, "x": tps // 2, "c": 2}
    here = {"z": zi, "y": yi, "x": lax.div(tp, 2), "c": lax.rem(tp, 2)}

    def at(**moves):
        c = {a: lax.rem(here[a] + moves[a], sizes[a]) if a in moves else here[a] for a in sizes}
        return {"sp": c["z"] * RING + c["y"], "tp": c["x"] * 2 + c["c"]}

    def steps(reach, axes):
        return [(a, m) for a in axes for m in sorted({r % sizes[a] for r in reach} - {0})]

    def greet(sem, moves, extra=()):
        for where in [at(**{a: m}) for a, m in moves] + list(extra):
            pl.semaphore_signal(sem, inc=1, device_id=where, device_id_type=MESH)
        return len(moves) + len(extra)

    def hear(sem, count):
        if count:
            pl.semaphore_wait(sem, count)

    near = steps((1, -1), "zyxc")
    met = [{"sp": nxt}, {"sp": prv}] + [at(**{a: m, "c": 1}) for a, m in steps((1, -1), "z")]
    barrier = pltpu.get_barrier_semaphore()
    heard = greet(barrier, near, met)

    before = HALO - SEG
    loads = []

    def load(src, dst):
        cp = pltpu.make_async_copy(src, dst, load_sem.at[len(loads)])
        cp.start()
        loads.append(cp)
        return cp

    def rows_in(ref, first, count):
        return ref.at[0, pl.ds(first, count)]

    tail = tokens - before
    k_last = load(rows_in(k_hbm, tail, before), kb.at[pl.ds(tokens, before)])
    v_last = load(rows_in(v_hbm, tail, before), vb.at[pl.ds(tokens, before)])
    firsts = [
        load(rows_in(q_hbm, 0, SEG), q0),
        load(rows_in(k_hbm, 0, SEG), kb.at[pl.ds(before, SEG)]),
        load(rows_in(g_hbm, 0, SEG), g0),
        load(rows_in(v_hbm, 0, SEG), vb.at[pl.ds(before, SEG)]),
    ]
    pl.semaphore_wait(barrier, heard)

    sent = []

    def send(src, dst, ssem, rsem, where):
        cp = pltpu.make_async_remote_copy(
            src_ref=src, dst_ref=dst, send_sem=ssem, recv_sem=rsem,
            device_id=where, device_id_type=MESH,
        )
        cp.start()
        sent.append(cp)
        return cp

    def lane_ds(h):
        return pl.ds(h * HEAD_DIM, HEAD_DIM)

    k_last.wait()
    v_last.wait()
    halo, ahead = {}, {}
    cuts = ((0, PAIR), (PAIR, before - PAIR))
    end = tokens + before
    for h in range(heads):
        for part in (1, 0):
            first, count = cuts[part]
            for a, band in enumerate((kb, vb)):
                n = len(halo)
                halo[h, a, part] = send(
                    band.at[pl.ds(tokens + first, count), lane_ds(h)], band.at[pl.ds(first, count), lane_ds(h)],
                    halo_send.at[n], halo_recv.at[n], {"sp": nxt},
                )
        if h == 0:
            for cp in firsts:
                cp.wait()
        for a, (src, dst, at_src, at_dst) in enumerate(
            ((q0, q, 0, tokens - SEG), (kb, kb, before, end), (g0, g, 0, tokens - SEG), (vb, vb, before, end))
        ):
            n = len(ahead)
            ahead[h, a] = send(
                src.at[pl.ds(at_src, SEG), lane_ds(h)], dst.at[pl.ds(at_dst, SEG), lane_ds(h)],
                ahead_send.at[n], ahead_recv.at[n], {"sp": prv},
            )

    heard = greet(round_sem.at[0], near)
    rb_all = load(rb_hbm, rb)
    rest = [
        load(rows_in(q_hbm, SEG, tokens - SEG), q.at[pl.ds(0, tokens - SEG)]),
        load(rows_in(k_hbm, SEG, tail - SEG), kb.at[pl.ds(HALO, tail - SEG)]),
        load(rows_in(g_hbm, SEG, tokens - SEG), g.at[pl.ds(0, tokens - SEG)]),
        load(rows_in(v_hbm, SEG, tail - SEG), vb.at[pl.ds(HALO, tail - SEG)]),
    ]

    scale = HEAD_DIM ** (-0.5)
    none_before = jnp.where(sp == 0, F32(NEG), F32(0.0))
    none_ahead = jnp.where(sp == ring - 1, F32(NEG), F32(0.0))
    rb_all.wait()
    rbs[...] = jnp.zeros_like(rbs)
    rbs[0:heads, 0:BUCKETS] = rb[...] * LOG2E
    lane = lax.broadcasted_iota(jnp.int32, (1, 2 * PAIR), 1)
    key_row = lax.broadcasted_iota(jnp.int32, (PAIR, PAIR), 0)
    q_col = lax.broadcasted_iota(jnp.int32, (PAIR, PAIR), 1)
    q_row = lax.broadcasted_iota(jnp.int32, (1, PAIR), 1)
    for h in range(heads):
        row = rbs[h : h + 1, :]
        last = rbs[h : h + 1, BUCKETS - 1 : BUCKETS]
        near = jnp.where(lane < BUCKETS, row, last)
        far = jnp.where((lane >= SEG) & (lane < BUCKETS), row, last)
        shape = (PAIR, 2 * PAIR)
        near = pltpu.roll(jnp.broadcast_to(near, shape), 193, 1, stride=1, stride_axis=0)[:, :PAIR]
        far = pltpu.roll(jnp.broadcast_to(far, shape), 65, 1, stride=1, stride_axis=0)[:, :PAIR]
        tab[h, 0:PAIR] = jnp.where((key_row < SEG) & (q_col >= SEG), NEG, last)
        tab[h, PAIR : 2 * PAIR] = far
        tab[h, 2 * PAIR : SPAN] = jnp.where((key_row >= SEG) & (q_col < SEG), NEG, near)

    for cp in rest:
        cp.wait()

    def block(h, p):
        ls = lanes_of(h)
        rows = slice(p * PAIR, p * PAIR + SPAN)
        cols = slice(p * PAIR, (p + 1) * PAIR)
        score = dot(kb[rows, ls], q[cols, ls], ((1,), (1,))) * (scale * LOG2E) + tab[h]
        outside = max(0, before - p * PAIR)
        if outside:
            score = jnp.concatenate([score[:outside] + none_before, score[outside:]], axis=0)
        if p == pairs - 1:
            seen = SPAN - SEG
            score = jnp.concatenate([score[:seen] + jnp.where(q_row >= SEG, none_ahead, 0.0), score[seen:]], axis=0)
        top = jnp.max(score, axis=0, keepdims=True)
        expo = jnp.exp2(score - top)
        prob = expo / jnp.sum(expo, axis=0, keepdims=True)
        pgrad = dot(vb[rows, ls], g[cols, ls], ((1,), (1,)))
        delta = jnp.sum(prob * pgrad, axis=0, keepdims=True)
        sgrad = prob * (pgrad - delta)
        pt[h, rows, cols] = prob.astype(BF16)
        st[h, rows, cols] = (sgrad * scale).astype(BF16)
        if p == pairs - 1:
            acc[h] = sgrad
        else:
            acc[h] += sgrad

    def key_side(h, kblock, terms, other):
        p0, p1 = max(0, kblock - 2), min(pairs - 1, kblock)
        span = slice(p0 * PAIR, (p1 + 1) * PAIR)
        rows = slice(kblock * PAIR, (kblock + 1) * PAIR)
        return dot(terms[h, rows, span], other[span, lanes_of(h)], ((1,), (0,)))

    def bias_row(h):
        base = SEG * h
        total = jnp.sum(acc[h, 0:PAIR], axis=0, keepdims=True)
        far = diagonal_sums(acc[h, PAIR : 2 * PAIR], 191 + base)
        near = diagonal_sums(acc[h, 2 * PAIR : SPAN], 63 + base)
        place = lane - base
        inner = (place >= SEG) & (place < BUCKETS)
        rest = jnp.where(inner, 0.0, far) + jnp.concatenate([total, jnp.zeros_like(total)], axis=1)
        rest = jnp.sum(rest, axis=1, keepdims=True)
        out = jnp.where((place >= 0) & (place < BUCKETS), near, 0.0) + jnp.where(inner, far, 0.0)
        return out + jnp.where(place == BUCKETS - 1, rest, 0.0)

    def query_side(h, p):
        rows = slice(p * PAIR, p * PAIR + SPAN)
        return dot(st[h, rows, p * PAIR : (p + 1) * PAIR], kb[rows, lanes_of(h)], ((0,), (0,)))

    def give_back(h):
        ls = lanes_of(h)
        for terms, other, out, part, m in ((st, q, out_k, part_k, 0), (pt, g, out_v, part_v, 1)):
            out[0:PAIR, ls] = key_side(h, 0, terms, other).astype(BF16)
            edge = key_side(h, 1, terms, other)
            out[PAIR:before, ls] = edge[:SEG].astype(BF16)
            part[0:SEG, ls] = edge[SEG:]
            edge = key_side(h, 4, terms, other)
            part[SEG:PAIR, ls] = edge[:SEG]
            fwd[m, :, ls] = edge[SEG:].astype(BF16)
        edge = query_side(h, pairs - 1)
        dq_ref[0, tokens - SEG : tokens, ls] = edge[:SEG].astype(BF16)
        fwd[2, :, ls] = edge[SEG:].astype(BF16)
        n = 2 * h
        pieces = [
            send(o.at[:, lane_ds(h)], i.at[:, lane_ds(h)], back_send.at[n + a], back_recv.at[n + a], {"sp": prv})
            for a, (o, i) in enumerate(((out_k, in_k), (out_v, in_v)))
        ]
        n = 3 * h
        return pieces + [
            send(fwd.at[a, :, lane_ds(h)], got.at[a, :, lane_ds(h)], fwd_send.at[n + a], fwd_recv.at[n + a], {"sp": nxt})
            for a in range(3)
        ]

    hear(round_sem.at[0], heard)
    heard = greet(round_sem.at[1], steps((2, -2), "zy"))
    back = []
    rows_of = []
    for h in range(heads):
        for a in range(4):
            ahead[h, a].wait_recv()
        block(h, pairs - 1)
        for p in range(pairs - 2, -1, -1):
            for a in range(2):
                halo[h, a, p].wait_recv()
            block(h, p)
        rows_of.append(bias_row(h))
        if h == 0:
            back += give_back(h)
    hear(round_sem.at[1], heard)
    heard = greet(round_sem.at[2], steps((1, 2, 3), "x"))

    def spread(buf, axes, rows, ssem, rsem, values):
        moves = [m for m in itertools.product(*(range(sizes[a]) for a in axes)) if any(m)]
        moves.sort(key=lambda m: -sum(min(v, sizes[a] - v) for a, v in zip(axes, m)))

        def slot(m):
            n = 0
            for a, v in zip(axes, m):
                n = n * sizes[a] + lax.rem(here[a] + v, sizes[a])
            return n

        mine = slot((0,) * len(axes))
        for r, value in enumerate(values):
            buf[mine, r : r + 1, :] = value
        part = pl.ds(0, rows)
        for n, m in enumerate(moves):
            send(buf.at[mine, part], buf.at[mine, part], ssem.at[n], rsem.at[mine], at(**dict(zip(axes, m))))

        def collect():
            for m in reversed(moves):
                other = buf.at[slot(m), part]
                pltpu.make_async_remote_copy(
                    src_ref=other, dst_ref=other, send_sem=ssem.at[0], recv_sem=rsem.at[slot(m)],
                    device_id=at(), device_id_type=MESH,
                ).wait_recv()

        return collect

    first, second = rows_of
    collect = spread(
        bz, "zc", 3, z_send, z_recv,
        [first[:, :PAIR], first[:, PAIR:] + second[:, :PAIR], second[:, PAIR:]],
    )
    back += give_back(heads - 1)

    for h in range(heads):
        ls = lanes_of(h)
        for p in range(pairs - 1):
            dq_ref[0, SEG + p * PAIR : SEG + (p + 1) * PAIR, ls] = query_side(h, p).astype(BF16)
        for terms, other, out in ((st, q, dk_ref), (pt, g, dv_ref)):
            out[0, SEG : SEG + PAIR, ls] = key_side(h, 2, terms, other).astype(BF16)

    collect()
    values = []
    for c in range(2):
        total = bz[c, 0:3]
        for z in range(1, zs):
            total += bz[2 * z + c, 0:3]
        values += [total[r : r + 1] for r in range(3)]
    hear(round_sem.at[2], heard)
    collect = spread(by, "yx", 6, y_send, y_recv, values)

    for h in range(heads):
        ls = lanes_of(h)
        for cp in back[5 * h : 5 * h + 5]:
            cp.wait_recv()
        dq_ref[0, 0:SEG, ls] = got[2, :, ls]
        for terms, other, out, part, come, m in ((st, q, dk_ref, part_k, in_k, 0), (pt, g, dv_ref, part_v, in_v, 1)):
            out[0, 0:SEG, ls] = (part[0:SEG, ls] + got[m, :, ls].astype(F32)).astype(BF16)
            mid = key_side(h, 3, terms, other) + come[0:PAIR, ls].astype(F32)
            out[0, tail : tail + PAIR, ls] = mid.astype(BF16)
            out[0, tokens - SEG : tokens, ls] = (part[SEG:PAIR, ls] + come[PAIR:before, ls].astype(F32)).astype(BF16)

    collect()
    xs = tps // 2
    for x in range(xs):
        total = by[x, 0:6]
        for y in range(1, RING):
            total += by[y * xs + x, 0:6]
        for c in range(2):
            r = 2 * (2 * x + c)
            low, mid, high = (total[3 * c + n : 3 * c + n + 1] for n in range(3))
            db_ref[r : r + 1, :PAIR] = low
            db_ref[r : r + 1, PAIR:] = mid[:, : BUCKETS - PAIR]
            both = pltpu.roll(jnp.concatenate([mid, high], axis=1), 2 * PAIR - SEG, 1)
            db_ref[r + 1 : r + 2, :PAIR] = both[:, :PAIR]
            db_ref[r + 1 : r + 2, PAIR:] = both[:, PAIR:BUCKETS]
    for cp in sent:
        cp.wait_send()


def put_out(*refs):
    ins, outs, sem = refs[:4], refs[4:8], refs[8]
    copies = [pltpu.make_async_copy(i, o, sem.at[n]) for n, (i, o) in enumerate(zip(ins, outs))]
    for cp in copies:
        cp.start()
    for cp in copies:
        cp.wait()


def local(queries, keys, values, rel_bias, out_grad):
    _, tokens, width = queries.shape
    heads = width // HEAD_DIM
    tps = lax.axis_size("tp")
    zs = lax.axis_size("sp") // RING
    band = tokens + HALO
    dma = pltpu.SemaphoreType.DMA
    grad = jax.ShapeDtypeStruct(queries.shape, BF16)
    anywhere = pl.BlockSpec(memory_space=pl.ANY)
    vmem = pl.BlockSpec(memory_space=pltpu.VMEM)
    bias = jax.ShapeDtypeStruct((heads * tps, BUCKETS), F32)
    outs = (grad, grad, grad, bias)
    held = pl.pallas_call(
        functools.partial(body, tokens, heads),
        out_shape=tuple(pltpu.VMEM(o.shape, o.dtype) for o in outs),
        in_specs=[anywhere] * 5,
        out_specs=(vmem, vmem, vmem, vmem),
        scratch_shapes=[
            pltpu.VMEM((tokens, width), BF16),
            pltpu.VMEM((tokens, width), BF16),
            pltpu.VMEM((SEG, width), BF16),
            pltpu.VMEM((SEG, width), BF16),
            pltpu.VMEM((band, width), BF16),
            pltpu.VMEM((band, width), BF16),
            pltpu.VMEM((heads, band, tokens), BF16),
            pltpu.VMEM((heads, band, tokens), BF16),
            pltpu.VMEM((heads, SPAN, PAIR), F32),
            pltpu.VMEM((heads, SPAN, PAIR), F32),
            pltpu.VMEM((8, 2 * PAIR), F32),
            pltpu.VMEM((heads, BUCKETS), F32),
            pltpu.VMEM((HALO - SEG, width), BF16),
            pltpu.VMEM((HALO - SEG, width), BF16),
            pltpu.VMEM((HALO - SEG, width), BF16),
            pltpu.VMEM((HALO - SEG, width), BF16),
            pltpu.VMEM((3, SEG, width), BF16),
            pltpu.VMEM((3, SEG, width), BF16),
            pltpu.VMEM((PAIR, width), F32),
            pltpu.VMEM((PAIR, width), F32),
            pltpu.VMEM((RING * tps // 2, 8, PAIR), F32),
            pltpu.VMEM((zs * 2, 8, PAIR), F32),
            pltpu.SemaphoreType.REGULAR((3,)),
            dma((11,)),
            dma((4 * heads,)),
            dma((4 * heads,)),
            dma((4 * heads,)),
            dma((4 * heads,)),
            dma((2 * heads,)),
            dma((2 * heads,)),
            dma((3 * heads,)),
            dma((3 * heads,)),
            dma((RING * tps // 2,)),
            dma((RING * tps // 2,)),
            dma((zs * 2,)),
            dma((zs * 2,)),
        ],
        compiler_params=pltpu.CompilerParams(collective_id=0, has_side_effects=True),
    )(queries, keys, values, rel_bias, out_grad)
    return pl.pallas_call(
        put_out,
        out_shape=outs,
        in_specs=[vmem] * 4,
        out_specs=(anywhere,) * 4,
        scratch_shapes=[dma((4,))],
    )(*[pltpu.with_memory_space_constraint(x, pltpu.VMEM) for x in held])


def solution(mesh):
    return jax.shard_map(
        local,
        mesh=mesh,
        in_specs=(
            P(None, "sp", "tp"),
            P(None, "sp", "tp"),
            P(None, "sp", "tp"),
            P("tp", None),
            P(None, "sp", "tp"),
        ),
        out_specs=(P(None, "sp", "tp"), P(None, "sp", "tp"), P(None, "sp", "tp"), P()),
        check_vma=False,
    )
```

```python
import functools
import itertools

import jax
import jax.numpy as jnp
from jax import lax
from jax.experimental import pallas as pl
from jax.experimental.pallas import tpu as pltpu
from jax.sharding import PartitionSpec as P

HEAD_DIM = 128
SEG = 64
LEFT = 4
BUCKETS = 192
HALO = LEFT * SEG
PAIR = 2 * SEG
SPAN = 3 * PAIR
NEG = -1e30
LOG2E = 1.4426950408889634
MESH = pl.DeviceIdType.MESH
F32 = jnp.float32
BF16 = jnp.bfloat16
RING = 8


def dot(a, b, contract):
    return lax.dot_general(a, b, (contract, ((), ())), preferred_element_type=F32)


def lanes_of(head):
    return slice(head * HEAD_DIM, (head + 1) * HEAD_DIM)


def diagonal_sums(x, offset):
    span = 2 * PAIR
    eight = jnp.zeros((8, span), F32)
    for r in range(0, x.shape[0], 8):
        eight += pltpu.roll(x[r : r + 8], (offset - r) % span, 1)
    row = lax.broadcasted_iota(jnp.int32, (8, span), 0)
    out = jnp.where(row == 0, eight, 0.0)
    for r in range(1, 8):
        out += jnp.where(row == r, pltpu.roll(eight, span - r, 1), 0.0)
    return jnp.sum(out, axis=0, keepdims=True)


def body(
    tokens, heads, q_hbm, k_hbm, v_hbm, rb_hbm, g_hbm,
    dq_ref, dk_ref, dv_ref, db_ref,
    q, g, q0, g0, kb, vb, pt, st, tab, acc, rbs, rb,
    out_k, out_v, in_k, in_v, fwd, got, part_k, part_v, by, bz, round_sem,
    load_sem, halo_send, halo_recv, ahead_send, ahead_recv,
    back_send, back_recv, fwd_send, fwd_recv,
    y_send, y_recv, z_send, z_recv,
):
    sp = lax.axis_index("sp")
    tp = lax.axis_index("tp")
    ring = lax.axis_size("sp")
    tps = lax.axis_size("tp")
    zs = ring // RING
    yi = lax.rem(sp, RING)
    zi = lax.div(sp, RING)
    nxt = lax.rem(sp + 1, ring)
    prv = lax.rem(sp + ring - 1, ring)
    pairs = tokens // PAIR

    sizes = {"z": zs, "y": RING, "x": tps // 2, "c": 2}
    here = {"z": zi, "y": yi, "x": lax.div(tp, 2), "c": lax.rem(tp, 2)}

    def at(**moves):
        c = {a: lax.rem(here[a] + moves[a], sizes[a]) if a in moves else here[a] for a in sizes}
        return {"sp": c["z"] * RING + c["y"], "tp": c["x"] * 2 + c["c"]}

    def steps(reach, axes):
        return [(a, m) for a in axes for m in sorted({r % sizes[a] for r in reach} - {0})]

    def greet(sem, moves, extra=()):
        for where in [at(**{a: m}) for a, m in moves] + list(extra):
            pl.semaphore_signal(sem, inc=1, device_id=where, device_id_type=MESH)
        return len(moves) + len(extra)

    def hear(sem, count):
        if count:
            pl.semaphore_wait(sem, count)

    near = steps((1, -1), "zyxc")
    met = [{"sp": nxt}, {"sp": prv}] + [at(**{a: m, "c": 1}) for a, m in steps((1, -1), "z")]
    barrier = pltpu.get_barrier_semaphore()
    heard = greet(barrier, near, met)

    before = HALO - SEG
    loads = []

    def load(src, dst):
        cp = pltpu.make_async_copy(src, dst, load_sem.at[len(loads)])
        cp.start()
        loads.append(cp)
        return cp

    def rows_in(ref, first, count):
        return ref.at[0, pl.ds(first, count)]

    tail = tokens - before
    k_last = load(rows_in(k_hbm, tail, before), kb.at[pl.ds(tokens, before)])
    v_last = load(rows_in(v_hbm, tail, before), vb.at[pl.ds(tokens, before)])
    firsts = [
        load(rows_in(q_hbm, 0, SEG), q0),
        load(rows_in(k_hbm, 0, SEG), kb.at[pl.ds(before, SEG)]),
        load(rows_in(g_hbm, 0, SEG), g0),
        load(rows_in(v_hbm, 0, SEG), vb.at[pl.ds(before, SEG)]),
    ]
    pl.semaphore_wait(barrier, heard)

    sent = []

    def send(src, dst, ssem, rsem, where):
        cp = pltpu.make_async_remote_copy(
            src_ref=src, dst_ref=dst, send_sem=ssem, recv_sem=rsem,
            device_id=where, device_id_type=MESH,
        )
        cp.start()
        sent.append(cp)
        return cp

    def lane_ds(h):
        return pl.ds(h * HEAD_DIM, HEAD_DIM)

    k_last.wait()
    v_last.wait()
    halo, ahead = {}, {}
    cuts = ((0, PAIR), (PAIR, before - PAIR))
    end = tokens + before
    for h in range(heads):
        for part in (1, 0):
            first, count = cuts[part]
            for a, band in enumerate((kb, vb)):
                n = len(halo)
                halo[h, a, part] = send(
                    band.at[pl.ds(tokens + first, count), lane_ds(h)], band.at[pl.ds(first, count), lane_ds(h)],
                    halo_send.at[n], halo_recv.at[n], {"sp": nxt},
                )
        if h == 0:
            for cp in firsts:
                cp.wait()
        for a, (src, dst, at_src, at_dst) in enumerate(
            ((q0, q, 0, tokens - SEG), (kb, kb, before, end), (g0, g, 0, tokens - SEG), (vb, vb, before, end))
        ):
            n = len(ahead)
            ahead[h, a] = send(
                src.at[pl.ds(at_src, SEG), lane_ds(h)], dst.at[pl.ds(at_dst, SEG), lane_ds(h)],
                ahead_send.at[n], ahead_recv.at[n], {"sp": prv},
            )

    heard = greet(round_sem.at[0], near)
    rb_all = load(rb_hbm, rb)
    rest = [
        load(rows_in(q_hbm, SEG, tokens - SEG), q.at[pl.ds(0, tokens - SEG)]),
        load(rows_in(k_hbm, SEG, tail - SEG), kb.at[pl.ds(HALO, tail - SEG)]),
        load(rows_in(g_hbm, SEG, tokens - SEG), g.at[pl.ds(0, tokens - SEG)]),
        load(rows_in(v_hbm, SEG, tail - SEG), vb.at[pl.ds(HALO, tail - SEG)]),
    ]

    scale = HEAD_DIM ** (-0.5)
    none_before = jnp.where(sp == 0, F32(NEG), F32(0.0))
    none_ahead = jnp.where(sp == ring - 1, F32(NEG), F32(0.0))
    rb_all.wait()
    rbs[...] = jnp.zeros_like(rbs)
    rbs[0:heads, 0:BUCKETS] = rb[...] * LOG2E
    lane = lax.broadcasted_iota(jnp.int32, (1, 2 * PAIR), 1)
    key_row = lax.broadcasted_iota(jnp.int32, (PAIR, PAIR), 0)
    q_col = lax.broadcasted_iota(jnp.int32, (PAIR, PAIR), 1)
    q_row = lax.broadcasted_iota(jnp.int32, (1, PAIR), 1)
    for h in range(heads):
        row = rbs[h : h + 1, :]
        last = rbs[h : h + 1, BUCKETS - 1 : BUCKETS]
        near = jnp.where(lane < BUCKETS, row, last)
        far = jnp.where((lane >= SEG) & (lane < BUCKETS), row, last)
        shape = (PAIR, 2 * PAIR)
        near = pltpu.roll(jnp.broadcast_to(near, shape), 193, 1, stride=1, stride_axis=0)[:, :PAIR]
        far = pltpu.roll(jnp.broadcast_to(far, shape), 65, 1, stride=1, stride_axis=0)[:, :PAIR]
        tab[h, 0:PAIR] = jnp.where((key_row < SEG) & (q_col >= SEG), NEG, last)
        tab[h, PAIR : 2 * PAIR] = far
        tab[h, 2 * PAIR : SPAN] = jnp.where((key_row >= SEG) & (q_col < SEG), NEG, near)

    for cp in rest:
        cp.wait()

    def block(h, p):
        ls = lanes_of(h)
        rows = slice(p * PAIR, p * PAIR + SPAN)
        cols = slice(p * PAIR, (p + 1) * PAIR)
        score = dot(kb[rows, ls], q[cols, ls], ((1,), (1,))) * (scale * LOG2E) + tab[h]
        outside = max(0, before - p * PAIR)
        if outside:
            score = jnp.concatenate([score[:outside] + none_before, score[outside:]], axis=0)
        if p == pairs - 1:
            seen = SPAN - SEG
            score = jnp.concatenate([score[:seen] + jnp.where(q_row >= SEG, none_ahead, 0.0), score[seen:]], axis=0)
        top = jnp.max(score, axis=0, keepdims=True)
        expo = jnp.exp2(score - top)
        prob = expo / jnp.sum(expo, axis=0, keepdims=True)
        pgrad = dot(vb[rows, ls], g[cols, ls], ((1,), (1,)))
        delta = jnp.sum(prob * pgrad, axis=0, keepdims=True)
        sgrad = prob * (pgrad - delta)
        pt[h, rows, cols] = prob.astype(BF16)
        st[h, rows, cols] = (sgrad * scale).astype(BF16)
        if p == pairs - 1:
            acc[h] = sgrad
        else:
            acc[h] += sgrad

    def key_side(h, kblock, terms, other):
        p0, p1 = max(0, kblock - 2), min(pairs - 1, kblock)
        span = slice(p0 * PAIR, (p1 + 1) * PAIR)
        rows = slice(kblock * PAIR, (kblock + 1) * PAIR)
        return dot(terms[h, rows, span], other[span, lanes_of(h)], ((1,), (0,)))

    def bias_row(h):
        base = SEG * h
        far = acc[h, PAIR : 2 * PAIR]
        clipped = key_row < q_col
        rest = acc[h, 0:PAIR] + jnp.where(clipped, far, 0.0)
        rest = jnp.sum(jnp.sum(rest, axis=0, keepdims=True), axis=1, keepdims=True)
        x = jnp.concatenate([acc[h, 2 * PAIR : SPAN], jnp.where(clipped, 0.0, far)], axis=1)
        return diagonal_sums(x, SEG - 1 + base) + jnp.where(lane == base + BUCKETS - 1, rest, 0.0)

    def query_side(h, p):
        rows = slice(p * PAIR, p * PAIR + SPAN)
        return dot(st[h, rows, p * PAIR : (p + 1) * PAIR], kb[rows, lanes_of(h)], ((0,), (0,)))

    def give_back(h):
        ls = lanes_of(h)
        for terms, other, out, part, m in ((st, q, out_k, part_k, 0), (pt, g, out_v, part_v, 1)):
            out[0:PAIR, ls] = key_side(h, 0, terms, other).astype(BF16)
            edge = key_side(h, 1, terms, other)
            out[PAIR:before, ls] = edge[:SEG].astype(BF16)
            part[0:SEG, ls] = edge[SEG:]
            edge = key_side(h, 4, terms, other)
            part[SEG:PAIR, ls] = edge[:SEG]
            fwd[m, :, ls] = edge[SEG:].astype(BF16)
        edge = query_side(h, pairs - 1)
        dq_ref[0, tokens - SEG : tokens, ls] = edge[:SEG].astype(BF16)
        fwd[2, :, ls] = edge[SEG:].astype(BF16)
        n = 2 * h
        pieces = [
            send(o.at[:, lane_ds(h)], i.at[:, lane_ds(h)], back_send.at[n + a], back_recv.at[n + a], {"sp": prv})
            for a, (o, i) in enumerate(((out_k, in_k), (out_v, in_v)))
        ]
        n = 3 * h
        return pieces + [
            send(fwd.at[a, :, lane_ds(h)], got.at[a, :, lane_ds(h)], fwd_send.at[n + a], fwd_recv.at[n + a], {"sp": nxt})
            for a in range(3)
        ]

    hear(round_sem.at[0], heard)
    heard = greet(round_sem.at[1], steps((2, -2), "zy"))
    back = []
    rows_of = []
    for h in range(heads):
        for a in range(4):
            ahead[h, a].wait_recv()
        block(h, pairs - 1)
        for p in range(pairs - 2, -1, -1):
            for a in range(2):
                halo[h, a, p].wait_recv()
            block(h, p)
        rows_of.append(bias_row(h))
        if h == 0:
            back += give_back(h)
    hear(round_sem.at[1], heard)
    heard = greet(round_sem.at[2], steps((1, 2, 3), "x"))

    def spread(buf, axes, rows, ssem, rsem, values):
        moves = [m for m in itertools.product(*(range(sizes[a]) for a in axes)) if any(m)]
        moves.sort(key=lambda m: -sum(min(v, sizes[a] - v) for a, v in zip(axes, m)))

        def slot(m):
            n = 0
            for a, v in zip(axes, m):
                n = n * sizes[a] + lax.rem(here[a] + v, sizes[a])
            return n

        mine = slot((0,) * len(axes))
        for r, value in enumerate(values):
            buf[mine, r : r + 1, :] = value
        part = pl.ds(0, rows)
        for n, m in enumerate(moves):
            send(buf.at[mine, part], buf.at[mine, part], ssem.at[n], rsem.at[mine], at(**dict(zip(axes, m))))

        def collect():
            for m in reversed(moves):
                other = buf.at[slot(m), part]
                pltpu.make_async_remote_copy(
                    src_ref=other, dst_ref=other, send_sem=ssem.at[0], recv_sem=rsem.at[slot(m)],
                    device_id=at(), device_id_type=MESH,
                ).wait_recv()

        return collect

    first, second = rows_of
    collect = spread(
        bz, "zc", 3, z_send, z_recv,
        [first[:, :PAIR], first[:, PAIR:] + second[:, :PAIR], second[:, PAIR:]],
    )
    back += give_back(heads - 1)

    for h in range(heads):
        ls = lanes_of(h)
        for p in range(pairs - 1):
            dq_ref[0, SEG + p * PAIR : SEG + (p + 1) * PAIR, ls] = query_side(h, p).astype(BF16)
        for terms, other, out in ((st, q, dk_ref), (pt, g, dv_ref)):
            out[0, SEG : SEG + PAIR, ls] = key_side(h, 2, terms, other).astype(BF16)

    collect()
    values = []
    for c in range(2):
        total = bz[c, 0:3]
        for z in range(1, zs):
            total += bz[2 * z + c, 0:3]
        values += [total[r : r + 1] for r in range(3)]
    hear(round_sem.at[2], heard)
    early = len(sent)
    collect = spread(by, "yx", 6, y_send, y_recv, values)

    for h in range(heads):
        ls = lanes_of(h)
        for cp in back[5 * h : 5 * h + 5]:
            cp.wait_recv()
        dq_ref[0, 0:SEG, ls] = got[2, :, ls]
        for terms, other, out, part, come, m in ((st, q, dk_ref, part_k, in_k, 0), (pt, g, dv_ref, part_v, in_v, 1)):
            out[0, 0:SEG, ls] = (part[0:SEG, ls] + got[m, :, ls].astype(F32)).astype(BF16)
            mid = key_side(h, 3, terms, other) + come[0:PAIR, ls].astype(F32)
            out[0, tail : tail + PAIR, ls] = mid.astype(BF16)
            out[0, tokens - SEG : tokens, ls] = (part[SEG:PAIR, ls] + come[PAIR:before, ls].astype(F32)).astype(BF16)

    for cp in sent[:early]:
        cp.wait_send()
    collect()
    xs = tps // 2
    for x in range(xs):
        total = by[x, 0:6]
        for y in range(1, RING):
            total += by[y * xs + x, 0:6]
        for c in range(2):
            r = 2 * (2 * x + c)
            low, mid, high = (total[3 * c + n : 3 * c + n + 1] for n in range(3))
            db_ref[r : r + 1, :PAIR] = low
            db_ref[r : r + 1, PAIR:] = mid[:, : BUCKETS - PAIR]
            both = pltpu.roll(jnp.concatenate([mid, high], axis=1), 2 * PAIR - SEG, 1)
            db_ref[r + 1 : r + 2, :PAIR] = both[:, :PAIR]
            db_ref[r + 1 : r + 2, PAIR:] = both[:, PAIR:BUCKETS]
    for cp in sent[early:]:
        cp.wait_send()


def put_out(*refs):
    ins, outs, sem = refs[:4], refs[4:8], refs[8]
    copies = [pltpu.make_async_copy(i, o, sem.at[n]) for n, (i, o) in enumerate(zip(ins, outs))]
    for cp in copies:
        cp.start()
    for cp in copies:
        cp.wait()


def local(queries, keys, values, rel_bias, out_grad):
    _, tokens, width = queries.shape
    heads = width // HEAD_DIM
    tps = lax.axis_size("tp")
    zs = lax.axis_size("sp") // RING
    band = tokens + HALO
    dma = pltpu.SemaphoreType.DMA
    grad = jax.ShapeDtypeStruct(queries.shape, BF16)
    anywhere = pl.BlockSpec(memory_space=pl.ANY)
    vmem = pl.BlockSpec(memory_space=pltpu.VMEM)
    bias = jax.ShapeDtypeStruct((heads * tps, BUCKETS), F32)
    outs = (grad, grad, grad, bias)
    held = pl.pallas_call(
        functools.partial(body, tokens, heads),
        out_shape=tuple(pltpu.VMEM(o.shape, o.dtype) for o in outs),
        in_specs=[anywhere] * 5,
        out_specs=(vmem, vmem, vmem, vmem),
        scratch_shapes=[
            pltpu.VMEM((tokens, width), BF16),
            pltpu.VMEM((tokens, width), BF16),
            pltpu.VMEM((SEG, width), BF16),
            pltpu.VMEM((SEG, width), BF16),
            pltpu.VMEM((band, width), BF16),
            pltpu.VMEM((band, width), BF16),
            pltpu.VMEM((heads, band, tokens), BF16),
            pltpu.VMEM((heads, band, tokens), BF16),
            pltpu.VMEM((heads, SPAN, PAIR), F32),
            pltpu.VMEM((heads, SPAN, PAIR), F32),
            pltpu.VMEM((8, 2 * PAIR), F32),
            pltpu.VMEM((heads, BUCKETS), F32),
            pltpu.VMEM((HALO - SEG, width), BF16),
            pltpu.VMEM((HALO - SEG, width), BF16),
            pltpu.VMEM((HALO - SEG, width), BF16),
            pltpu.VMEM((HALO - SEG, width), BF16),
            pltpu.VMEM((3, SEG, width), BF16),
            pltpu.VMEM((3, SEG, width), BF16),
            pltpu.VMEM((PAIR, width), F32),
            pltpu.VMEM((PAIR, width), F32),
            pltpu.VMEM((RING * tps // 2, 8, PAIR), F32),
            pltpu.VMEM((zs * 2, 8, PAIR), F32),
            pltpu.SemaphoreType.REGULAR((3,)),
            dma((11,)),
            dma((4 * heads,)),
            dma((4 * heads,)),
            dma((4 * heads,)),
            dma((4 * heads,)),
            dma((2 * heads,)),
            dma((2 * heads,)),
            dma((3 * heads,)),
            dma((3 * heads,)),
            dma((RING * tps // 2,)),
            dma((RING * tps // 2,)),
            dma((zs * 2,)),
            dma((zs * 2,)),
        ],
        compiler_params=pltpu.CompilerParams(collective_id=0, has_side_effects=True),
    )(queries, keys, values, rel_bias, out_grad)
    return pl.pallas_call(
        put_out,
        out_shape=outs,
        in_specs=[vmem] * 4,
        out_specs=(anywhere,) * 4,
        scratch_shapes=[dma((4,))],
    )(*[pltpu.with_memory_space_constraint(x, pltpu.VMEM) for x in held])


def solution(mesh):
    return jax.shard_map(
        local,
        mesh=mesh,
        in_specs=(
            P(None, "sp", "tp"),
            P(None, "sp", "tp"),
            P(None, "sp", "tp"),
            P("tp", None),
            P(None, "sp", "tp"),
        ),
        out_specs=(P(None, "sp", "tp"), P(None, "sp", "tp"), P(None, "sp", "tp"), P()),
        check_vma=False,
    )
```

```python
import functools
import itertools

import jax
import jax.numpy as jnp
from jax import lax
from jax.experimental import pallas as pl
from jax.experimental.pallas import tpu as pltpu
from jax.sharding import PartitionSpec as P

HEAD_DIM = 128
SEG = 64
LEFT = 4
BUCKETS = 192
HALO = LEFT * SEG
PAIR = 2 * SEG
SPAN = 3 * PAIR
NEG = -1e30
LOG2E = 1.4426950408889634
MESH = pl.DeviceIdType.MESH
F32 = jnp.float32
BF16 = jnp.bfloat16
RING = 8


def dot(a, b, contract):
    return lax.dot_general(a, b, (contract, ((), ())), preferred_element_type=F32)


def lanes_of(head):
    return slice(head * HEAD_DIM, (head + 1) * HEAD_DIM)


def diagonal_sums(x, offset):
    span = 2 * PAIR
    eight = jnp.zeros((8, span), F32)
    for r in range(0, x.shape[0], 8):
        eight += pltpu.roll(x[r : r + 8], (offset - r) % span, 1)
    row = lax.broadcasted_iota(jnp.int32, (8, span), 0)
    out = jnp.where(row == 0, eight, 0.0)
    for r in range(1, 8):
        out += jnp.where(row == r, pltpu.roll(eight, span - r, 1), 0.0)
    return jnp.sum(out, axis=0, keepdims=True)


def body(
    tokens, heads, q_hbm, k_hbm, v_hbm, rb_hbm, g_hbm,
    dq_ref, dk_ref, dv_ref, db_ref,
    q, g, q0, g0, kb, vb, pt, st, tab, acc, rbs, rb,
    out_k, out_v, in_k, in_v, fwd, got, part_k, part_v, by, bz, round_sem,
    load_sem, halo_send, halo_recv, ahead_send, ahead_recv,
    back_send, back_recv, fwd_send, fwd_recv,
    y_send, y_recv, z_send, z_recv,
):
    sp = lax.axis_index("sp")
    tp = lax.axis_index("tp")
    ring = lax.axis_size("sp")
    tps = lax.axis_size("tp")
    zs = ring // RING
    yi = lax.rem(sp, RING)
    zi = lax.div(sp, RING)
    nxt = lax.rem(sp + 1, ring)
    prv = lax.rem(sp + ring - 1, ring)
    pairs = tokens // PAIR

    sizes = {"z": zs, "y": RING, "x": tps // 2, "c": 2}
    here = {"z": zi, "y": yi, "x": lax.div(tp, 2), "c": lax.rem(tp, 2)}

    def at(**moves):
        c = {a: lax.rem(here[a] + moves[a], sizes[a]) if a in moves else here[a] for a in sizes}
        return {"sp": c["z"] * RING + c["y"], "tp": c["x"] * 2 + c["c"]}

    def steps(reach, axes):
        return [(a, m) for a in axes for m in sorted({r % sizes[a] for r in reach} - {0})]

    def greet(sem, moves, extra=()):
        for where in [at(**{a: m}) for a, m in moves] + list(extra):
            pl.semaphore_signal(sem, inc=1, device_id=where, device_id_type=MESH)
        return len(moves) + len(extra)

    def hear(sem, count):
        if count:
            pl.semaphore_wait(sem, count)

    near = steps((1, -1), "zyxc")
    met = [{"sp": nxt}, {"sp": prv}] + [at(**{a: m, "c": 1}) for a, m in steps((1, -1), "z")]
    barrier = pltpu.get_barrier_semaphore()
    heard = greet(barrier, near, met)

    before = HALO - SEG
    loads = []

    def load(src, dst):
        cp = pltpu.make_async_copy(src, dst, load_sem.at[len(loads)])
        cp.start()
        loads.append(cp)
        return cp

    def rows_in(ref, first, count):
        return ref.at[0, pl.ds(first, count)]

    tail = tokens - before
    k_last = load(rows_in(k_hbm, tail, before), kb.at[pl.ds(tokens, before)])
    v_last = load(rows_in(v_hbm, tail, before), vb.at[pl.ds(tokens, before)])
    firsts = [
        load(rows_in(q_hbm, 0, SEG), q0),
        load(rows_in(k_hbm, 0, SEG), kb.at[pl.ds(before, SEG)]),
        load(rows_in(g_hbm, 0, SEG), g0),
        load(rows_in(v_hbm, 0, SEG), vb.at[pl.ds(before, SEG)]),
    ]
    pl.semaphore_wait(barrier, heard)

    sent = []

    def send(src, dst, ssem, rsem, where):
        cp = pltpu.make_async_remote_copy(
            src_ref=src, dst_ref=dst, send_sem=ssem, recv_sem=rsem,
            device_id=where, device_id_type=MESH,
        )
        cp.start()
        sent.append(cp)
        return cp

    def lane_ds(h):
        return pl.ds(h * HEAD_DIM, HEAD_DIM)

    k_last.wait()
    v_last.wait()
    halo, ahead = {}, {}
    cuts = ((0, PAIR), (PAIR, before - PAIR))
    end = tokens + before
    for h in range(heads):
        for part in (1, 0):
            first, count = cuts[part]
            for a, band in enumerate((kb, vb)):
                n = len(halo)
                halo[h, a, part] = send(
                    band.at[pl.ds(tokens + first, count), lane_ds(h)], band.at[pl.ds(first, count), lane_ds(h)],
                    halo_send.at[n], halo_recv.at[n], {"sp": nxt},
                )
        if h == 0:
            for cp in firsts:
                cp.wait()
        for a, (src, dst, at_src, at_dst) in enumerate(
            ((q0, q, 0, tokens - SEG), (kb, kb, before, end), (g0, g, 0, tokens - SEG), (vb, vb, before, end))
        ):
            n = len(ahead)
            ahead[h, a] = send(
                src.at[pl.ds(at_src, SEG), lane_ds(h)], dst.at[pl.ds(at_dst, SEG), lane_ds(h)],
                ahead_send.at[n], ahead_recv.at[n], {"sp": prv},
            )

    heard = greet(round_sem.at[0], near)
    rb_all = load(rb_hbm, rb)
    rest = [
        load(rows_in(q_hbm, SEG, tokens - SEG), q.at[pl.ds(0, tokens - SEG)]),
        load(rows_in(k_hbm, SEG, tail - SEG), kb.at[pl.ds(HALO, tail - SEG)]),
        load(rows_in(g_hbm, SEG, tokens - SEG), g.at[pl.ds(0, tokens - SEG)]),
        load(rows_in(v_hbm, SEG, tail - SEG), vb.at[pl.ds(HALO, tail - SEG)]),
    ]

    scale = HEAD_DIM ** (-0.5)
    none_before = jnp.where(sp == 0, F32(NEG), F32(0.0))
    none_ahead = jnp.where(sp == ring - 1, F32(NEG), F32(0.0))
    rb_all.wait()
    rbs[...] = jnp.zeros_like(rbs)
    rbs[0:heads, 0:BUCKETS] = rb[...] * LOG2E
    lane = lax.broadcasted_iota(jnp.int32, (1, 2 * PAIR), 1)
    key_row = lax.broadcasted_iota(jnp.int32, (PAIR, PAIR), 0)
    q_col = lax.broadcasted_iota(jnp.int32, (PAIR, PAIR), 1)
    q_row = lax.broadcasted_iota(jnp.int32, (1, PAIR), 1)
    for h in range(heads):
        row = rbs[h : h + 1, :]
        last = rbs[h : h + 1, BUCKETS - 1 : BUCKETS]
        near = jnp.where(lane < BUCKETS, row, last)
        far = jnp.where((lane >= SEG) & (lane < BUCKETS), row, last)
        shape = (PAIR, 2 * PAIR)
        near = pltpu.roll(jnp.broadcast_to(near, shape), 193, 1, stride=1, stride_axis=0)[:, :PAIR]
        far = pltpu.roll(jnp.broadcast_to(far, shape), 65, 1, stride=1, stride_axis=0)[:, :PAIR]
        tab[h, 0:PAIR] = jnp.where((key_row < SEG) & (q_col >= SEG), NEG, last)
        tab[h, PAIR : 2 * PAIR] = far
        tab[h, 2 * PAIR : SPAN] = jnp.where((key_row >= SEG) & (q_col < SEG), NEG, near)

    for cp in rest:
        cp.wait()

    def block(h, p):
        ls = lanes_of(h)
        rows = slice(p * PAIR, p * PAIR + SPAN)
        cols = slice(p * PAIR, (p + 1) * PAIR)
        score = dot(kb[rows, ls], q[cols, ls], ((1,), (1,))) * (scale * LOG2E) + tab[h]
        outside = max(0, before - p * PAIR)
        if outside:
            score = jnp.concatenate([score[:outside] + none_before, score[outside:]], axis=0)
        if p == pairs - 1:
            seen = SPAN - SEG
            score = jnp.concatenate([score[:seen] + jnp.where(q_row >= SEG, none_ahead, 0.0), score[seen:]], axis=0)
        top = jnp.max(score, axis=0, keepdims=True)
        expo = jnp.exp2(score - top)
        prob = expo / jnp.sum(expo, axis=0, keepdims=True)
        pgrad = dot(vb[rows, ls], g[cols, ls], ((1,), (1,)))
        delta = jnp.sum(prob * pgrad, axis=0, keepdims=True)
        sgrad = prob * (pgrad - delta)
        pt[h, rows, cols] = prob.astype(BF16)
        st[h, rows, cols] = (sgrad * scale).astype(BF16)
        if p == pairs - 1:
            acc[h] = sgrad
        else:
            acc[h] += sgrad

    def key_side(h, kblock, terms, other):
        p0, p1 = max(0, kblock - 2), min(pairs - 1, kblock)
        span = slice(p0 * PAIR, (p1 + 1) * PAIR)
        rows = slice(kblock * PAIR, (kblock + 1) * PAIR)
        return dot(terms[h, rows, span], other[span, lanes_of(h)], ((1,), (0,)))

    def bias_row(h):
        base = SEG * h
        far = acc[h, PAIR : 2 * PAIR]
        clipped = key_row < q_col
        rest = acc[h, 0:PAIR] + jnp.where(clipped, far, 0.0)
        rest = jnp.sum(jnp.sum(rest, axis=0, keepdims=True), axis=1, keepdims=True)
        x = jnp.concatenate([acc[h, 2 * PAIR : SPAN], jnp.where(clipped, 0.0, far)], axis=1)
        return diagonal_sums(x, SEG - 1 + base) + jnp.where(lane == base + BUCKETS - 1, rest, 0.0)

    def query_side(h, p):
        rows = slice(p * PAIR, p * PAIR + SPAN)
        return dot(st[h, rows, p * PAIR : (p + 1) * PAIR], kb[rows, lanes_of(h)], ((0,), (0,)))

    def give_back(h):
        ls = lanes_of(h)
        for terms, other, out, part, m in ((st, q, out_k, part_k, 0), (pt, g, out_v, part_v, 1)):
            out[0:PAIR, ls] = key_side(h, 0, terms, other).astype(BF16)
            edge = key_side(h, 1, terms, other)
            out[PAIR:before, ls] = edge[:SEG].astype(BF16)
            part[0:SEG, ls] = edge[SEG:]
            edge = key_side(h, 4, terms, other)
            part[SEG:PAIR, ls] = edge[:SEG]
            fwd[m, :, ls] = edge[SEG:].astype(BF16)
        edge = query_side(h, pairs - 1)
        dq_ref[0, tokens - SEG : tokens, ls] = edge[:SEG].astype(BF16)
        fwd[2, :, ls] = edge[SEG:].astype(BF16)
        n = 2 * h
        pieces = [
            send(o.at[:, lane_ds(h)], i.at[:, lane_ds(h)], back_send.at[n + a], back_recv.at[n + a], {"sp": prv})
            for a, (o, i) in enumerate(((out_k, in_k), (out_v, in_v)))
        ]
        n = 3 * h
        return pieces + [
            send(fwd.at[a, :, lane_ds(h)], got.at[a, :, lane_ds(h)], fwd_send.at[n + a], fwd_recv.at[n + a], {"sp": nxt})
            for a in range(3)
        ]

    hear(round_sem.at[0], heard)
    heard = greet(round_sem.at[1], steps((2, -2), "zy"))
    back = []
    rows_of = []
    for h in range(heads):
        for a in range(4):
            ahead[h, a].wait_recv()
        block(h, pairs - 1)
        for p in range(pairs - 2, -1, -1):
            if h and p == 0:
                rows_of.append(bias_row(h - 1))
                back += give_back(h - 1)
            for a in range(2):
                halo[h, a, p].wait_recv()
            block(h, p)
    rows_of.append(bias_row(heads - 1))
    hear(round_sem.at[1], heard)
    heard = greet(round_sem.at[2], steps((1, 2, 3), "x"))

    def spread(buf, axes, rows, ssem, rsem, values):
        moves = [m for m in itertools.product(*(range(sizes[a]) for a in axes)) if any(m)]
        moves.sort(key=lambda m: -sum(min(v, sizes[a] - v) for a, v in zip(axes, m)))

        def slot(m):
            n = 0
            for a, v in zip(axes, m):
                n = n * sizes[a] + lax.rem(here[a] + v, sizes[a])
            return n

        mine = slot((0,) * len(axes))
        for r, value in enumerate(values):
            buf[mine, r : r + 1, :] = value
        part = pl.ds(0, rows)
        for n, m in enumerate(moves):
            send(buf.at[mine, part], buf.at[mine, part], ssem.at[n], rsem.at[mine], at(**dict(zip(axes, m))))

        def collect():
            for m in reversed(moves):
                other = buf.at[slot(m), part]
                pltpu.make_async_remote_copy(
                    src_ref=other, dst_ref=other, send_sem=ssem.at[0], recv_sem=rsem.at[slot(m)],
                    device_id=at(), device_id_type=MESH,
                ).wait_recv()

        return collect

    first, second = rows_of
    collect = spread(
        bz, "zc", 3, z_send, z_recv,
        [first[:, :PAIR], first[:, PAIR:] + second[:, :PAIR], second[:, PAIR:]],
    )
    back += give_back(heads - 1)

    for h in range(heads):
        ls = lanes_of(h)
        for p in range(pairs - 1):
            dq_ref[0, SEG + p * PAIR : SEG + (p + 1) * PAIR, ls] = query_side(h, p).astype(BF16)
        for terms, other, out in ((st, q, dk_ref), (pt, g, dv_ref)):
            out[0, SEG : SEG + PAIR, ls] = key_side(h, 2, terms, other).astype(BF16)

    collect()
    values = []
    for c in range(2):
        total = bz[c, 0:3]
        for z in range(1, zs):
            total += bz[2 * z + c, 0:3]
        values += [total[r : r + 1] for r in range(3)]
    hear(round_sem.at[2], heard)
    early = len(sent)
    collect = spread(by, "yx", 6, y_send, y_recv, values)

    for h in range(heads):
        ls = lanes_of(h)
        for cp in back[5 * h : 5 * h + 5]:
            cp.wait_recv()
        dq_ref[0, 0:SEG, ls] = got[2, :, ls]
        for terms, other, out, part, come, m in ((st, q, dk_ref, part_k, in_k, 0), (pt, g, dv_ref, part_v, in_v, 1)):
            out[0, 0:SEG, ls] = (part[0:SEG, ls] + got[m, :, ls].astype(F32)).astype(BF16)
            mid = key_side(h, 3, terms, other) + come[0:PAIR, ls].astype(F32)
            out[0, tail : tail + PAIR, ls] = mid.astype(BF16)
            out[0, tokens - SEG : tokens, ls] = (part[SEG:PAIR, ls] + come[PAIR:before, ls].astype(F32)).astype(BF16)

    for cp in sent[:early]:
        cp.wait_send()
    collect()
    xs = tps // 2
    for x in range(xs):
        total = by[x, 0:6]
        for y in range(1, RING):
            total += by[y * xs + x, 0:6]
        for c in range(2):
            r = 2 * (2 * x + c)
            low, mid, high = (total[3 * c + n : 3 * c + n + 1] for n in range(3))
            db_ref[r : r + 1, :PAIR] = low
            db_ref[r : r + 1, PAIR:] = mid[:, : BUCKETS - PAIR]
            both = pltpu.roll(jnp.concatenate([mid, high], axis=1), 2 * PAIR - SEG, 1)
            db_ref[r + 1 : r + 2, :PAIR] = both[:, :PAIR]
            db_ref[r + 1 : r + 2, PAIR:] = both[:, PAIR:BUCKETS]
    for cp in sent[early:]:
        cp.wait_send()


def put_out(*refs):
    ins, outs, sem = refs[:4], refs[4:8], refs[8]
    copies = [pltpu.make_async_copy(i, o, sem.at[n]) for n, (i, o) in enumerate(zip(ins, outs))]
    for cp in copies:
        cp.start()
    for cp in copies:
        cp.wait()


def local(queries, keys, values, rel_bias, out_grad):
    _, tokens, width = queries.shape
    heads = width // HEAD_DIM
    tps = lax.axis_size("tp")
    zs = lax.axis_size("sp") // RING
    band = tokens + HALO
    dma = pltpu.SemaphoreType.DMA
    grad = jax.ShapeDtypeStruct(queries.shape, BF16)
    anywhere = pl.BlockSpec(memory_space=pl.ANY)
    vmem = pl.BlockSpec(memory_space=pltpu.VMEM)
    bias = jax.ShapeDtypeStruct((heads * tps, BUCKETS), F32)
    outs = (grad, grad, grad, bias)
    held = pl.pallas_call(
        functools.partial(body, tokens, heads),
        out_shape=tuple(pltpu.VMEM(o.shape, o.dtype) for o in outs),
        in_specs=[anywhere] * 5,
        out_specs=(vmem, vmem, vmem, vmem),
        scratch_shapes=[
            pltpu.VMEM((tokens, width), BF16),
            pltpu.VMEM((tokens, width), BF16),
            pltpu.VMEM((SEG, width), BF16),
            pltpu.VMEM((SEG, width), BF16),
            pltpu.VMEM((band, width), BF16),
            pltpu.VMEM((band, width), BF16),
            pltpu.VMEM((heads, band, tokens), BF16),
            pltpu.VMEM((heads, band, tokens), BF16),
            pltpu.VMEM((heads, SPAN, PAIR), F32),
            pltpu.VMEM((heads, SPAN, PAIR), F32),
            pltpu.VMEM((8, 2 * PAIR), F32),
            pltpu.VMEM((heads, BUCKETS), F32),
            pltpu.VMEM((HALO - SEG, width), BF16),
            pltpu.VMEM((HALO - SEG, width), BF16),
            pltpu.VMEM((HALO - SEG, width), BF16),
            pltpu.VMEM((HALO - SEG, width), BF16),
            pltpu.VMEM((3, SEG, width), BF16),
            pltpu.VMEM((3, SEG, width), BF16),
            pltpu.VMEM((PAIR, width), F32),
            pltpu.VMEM((PAIR, width), F32),
            pltpu.VMEM((RING * tps // 2, 8, PAIR), F32),
            pltpu.VMEM((zs * 2, 8, PAIR), F32),
            pltpu.SemaphoreType.REGULAR((3,)),
            dma((11,)),
            dma((4 * heads,)),
            dma((4 * heads,)),
            dma((4 * heads,)),
            dma((4 * heads,)),
            dma((2 * heads,)),
            dma((2 * heads,)),
            dma((3 * heads,)),
            dma((3 * heads,)),
            dma((RING * tps // 2,)),
            dma((RING * tps // 2,)),
            dma((zs * 2,)),
            dma((zs * 2,)),
        ],
        compiler_params=pltpu.CompilerParams(collective_id=0, has_side_effects=True),
    )(queries, keys, values, rel_bias, out_grad)
    return pl.pallas_call(
        put_out,
        out_shape=outs,
        in_specs=[vmem] * 4,
        out_specs=(anywhere,) * 4,
        scratch_shapes=[dma((4,))],
    )(*[pltpu.with_memory_space_constraint(x, pltpu.VMEM) for x in held])


def solution(mesh):
    return jax.shard_map(
        local,
        mesh=mesh,
        in_specs=(
            P(None, "sp", "tp"),
            P(None, "sp", "tp"),
            P(None, "sp", "tp"),
            P("tp", None),
            P(None, "sp", "tp"),
        ),
        out_specs=(P(None, "sp", "tp"), P(None, "sp", "tp"), P(None, "sp", "tp"), P()),
        check_vma=False,
    )
```

```python
import functools
import itertools

import jax
import jax.numpy as jnp
from jax import lax
from jax.experimental import pallas as pl
from jax.experimental.pallas import tpu as pltpu
from jax.sharding import PartitionSpec as P

HEAD_DIM = 128
SEG = 64
LEFT = 4
BUCKETS = 192
HALO = LEFT * SEG
PAIR = 2 * SEG
SPAN = 3 * PAIR
NEG = -1e30
LOG2E = 1.4426950408889634
MESH = pl.DeviceIdType.MESH
F32 = jnp.float32
BF16 = jnp.bfloat16
RING = 8


def dot(a, b, contract):
    return lax.dot_general(a, b, (contract, ((), ())), preferred_element_type=F32)


def lanes_of(head):
    return slice(head * HEAD_DIM, (head + 1) * HEAD_DIM)


def diagonal_sums(x, offset):
    span = 2 * PAIR
    eight = jnp.zeros((8, span), F32)
    for r in range(0, x.shape[0], 8):
        eight += pltpu.roll(x[r : r + 8], (offset - r) % span, 1)
    row = lax.broadcasted_iota(jnp.int32, (8, span), 0)
    out = jnp.where(row == 0, eight, 0.0)
    for r in range(1, 8):
        out += jnp.where(row == r, pltpu.roll(eight, span - r, 1), 0.0)
    return jnp.sum(out, axis=0, keepdims=True)


def body(
    tokens, heads, q_hbm, k_hbm, v_hbm, rb_hbm, g_hbm,
    dq_ref, dk_ref, dv_ref, db_ref,
    q, g, q0, g0, kb, vb, pt, st, tab, acc, rbs, rb,
    out_k, out_v, in_k, in_v, fwd, got, part_k, part_v, by, bz, round_sem,
    load_sem, halo_send, halo_recv, ahead_send, ahead_recv,
    back_send, back_recv, fwd_send, fwd_recv,
    y_send, y_recv, z_send, z_recv,
):
    sp = lax.axis_index("sp")
    tp = lax.axis_index("tp")
    ring = lax.axis_size("sp")
    tps = lax.axis_size("tp")
    zs = ring // RING
    yi = lax.rem(sp, RING)
    zi = lax.div(sp, RING)
    nxt = lax.rem(sp + 1, ring)
    prv = lax.rem(sp + ring - 1, ring)
    pairs = tokens // PAIR

    sizes = {"z": zs, "y": RING, "x": tps // 2, "c": 2}
    here = {"z": zi, "y": yi, "x": lax.div(tp, 2), "c": lax.rem(tp, 2)}

    def at(**moves):
        c = {a: lax.rem(here[a] + moves[a], sizes[a]) if a in moves else here[a] for a in sizes}
        return {"sp": c["z"] * RING + c["y"], "tp": c["x"] * 2 + c["c"]}

    def steps(reach, axes):
        return [(a, m) for a in axes for m in sorted({r % sizes[a] for r in reach} - {0})]

    def greet(sem, moves, extra=()):
        for where in [at(**{a: m}) for a, m in moves] + list(extra):
            pl.semaphore_signal(sem, inc=1, device_id=where, device_id_type=MESH)
        return len(moves) + len(extra)

    def hear(sem, count):
        if count:
            pl.semaphore_wait(sem, count)

    near = steps((1, -1), "zyxc")
    met = [{"sp": nxt}, {"sp": prv}] + [at(**{a: m, "c": 1}) for a, m in steps((1, -1), "z")]
    barrier = pltpu.get_barrier_semaphore()
    heard = greet(barrier, near, met)

    before = HALO - SEG
    loads = []

    def load(src, dst):
        cp = pltpu.make_async_copy(src, dst, load_sem.at[len(loads)])
        cp.start()
        loads.append(cp)
        return cp

    def rows_in(ref, first, count):
        return ref.at[0, pl.ds(first, count)]

    tail = tokens - before
    k_last = load(rows_in(k_hbm, tail, before), kb.at[pl.ds(tokens, before)])
    v_last = load(rows_in(v_hbm, tail, before), vb.at[pl.ds(tokens, before)])
    firsts = [
        load(rows_in(q_hbm, 0, SEG), q0),
        load(rows_in(k_hbm, 0, SEG), kb.at[pl.ds(before, SEG)]),
        load(rows_in(g_hbm, 0, SEG), g0),
        load(rows_in(v_hbm, 0, SEG), vb.at[pl.ds(before, SEG)]),
    ]
    pl.semaphore_wait(barrier, heard)

    sent = []

    def send(src, dst, ssem, rsem, where):
        cp = pltpu.make_async_remote_copy(
            src_ref=src, dst_ref=dst, send_sem=ssem, recv_sem=rsem,
            device_id=where, device_id_type=MESH,
        )
        cp.start()
        sent.append(cp)
        return cp

    def lane_ds(h):
        return pl.ds(h * HEAD_DIM, HEAD_DIM)

    k_last.wait()
    v_last.wait()
    halo, ahead = {}, {}
    cuts = ((0, PAIR), (PAIR, before - PAIR))
    end = tokens + before
    for h in range(heads):
        for part in (1, 0):
            first, count = cuts[part]
            for a, band in enumerate((kb, vb)):
                n = len(halo)
                halo[h, a, part] = send(
                    band.at[pl.ds(tokens + first, count), lane_ds(h)], band.at[pl.ds(first, count), lane_ds(h)],
                    halo_send.at[n], halo_recv.at[n], {"sp": nxt},
                )
        if h == 0:
            for cp in firsts:
                cp.wait()
        for a, (src, dst, at_src, at_dst) in enumerate(
            ((q0, q, 0, tokens - SEG), (kb, kb, before, end), (g0, g, 0, tokens - SEG), (vb, vb, before, end))
        ):
            n = len(ahead)
            ahead[h, a] = send(
                src.at[pl.ds(at_src, SEG), lane_ds(h)], dst.at[pl.ds(at_dst, SEG), lane_ds(h)],
                ahead_send.at[n], ahead_recv.at[n], {"sp": prv},
            )

    heard = greet(round_sem.at[0], near)
    rb_all = load(rb_hbm, rb)
    rest = [
        load(rows_in(q_hbm, SEG, tokens - SEG), q.at[pl.ds(0, tokens - SEG)]),
        load(rows_in(k_hbm, SEG, tail - SEG), kb.at[pl.ds(HALO, tail - SEG)]),
        load(rows_in(g_hbm, SEG, tokens - SEG), g.at[pl.ds(0, tokens - SEG)]),
        load(rows_in(v_hbm, SEG, tail - SEG), vb.at[pl.ds(HALO, tail - SEG)]),
    ]

    scale = HEAD_DIM ** (-0.5)
    none_before = jnp.where(sp == 0, F32(NEG), F32(0.0))
    none_ahead = jnp.where(sp == ring - 1, F32(NEG), F32(0.0))
    rb_all.wait()
    rbs[...] = jnp.zeros_like(rbs)
    rbs[0:heads, 0:BUCKETS] = rb[...] * LOG2E
    lane = lax.broadcasted_iota(jnp.int32, (1, 2 * PAIR), 1)
    key_row = lax.broadcasted_iota(jnp.int32, (PAIR, PAIR), 0)
    q_col = lax.broadcasted_iota(jnp.int32, (PAIR, PAIR), 1)
    q_row = lax.broadcasted_iota(jnp.int32, (1, PAIR), 1)
    for h in range(heads):
        row = rbs[h : h + 1, :]
        last = rbs[h : h + 1, BUCKETS - 1 : BUCKETS]
        near = jnp.where(lane < BUCKETS, row, last)
        far = jnp.where((lane >= SEG) & (lane < BUCKETS), row, last)
        shape = (PAIR, 2 * PAIR)
        near = pltpu.roll(jnp.broadcast_to(near, shape), 193, 1, stride=1, stride_axis=0)[:, :PAIR]
        far = pltpu.roll(jnp.broadcast_to(far, shape), 65, 1, stride=1, stride_axis=0)[:, :PAIR]
        tab[h, 0:PAIR] = jnp.where((key_row < SEG) & (q_col >= SEG), NEG, last)
        tab[h, PAIR : 2 * PAIR] = far
        tab[h, 2 * PAIR : SPAN] = jnp.where((key_row >= SEG) & (q_col < SEG), NEG, near)

    for cp in rest:
        cp.wait()

    def block(h, p):
        ls = lanes_of(h)
        rows = slice(p * PAIR, p * PAIR + SPAN)
        cols = slice(p * PAIR, (p + 1) * PAIR)
        score = dot(kb[rows, ls], q[cols, ls], ((1,), (1,))) * (scale * LOG2E) + tab[h]
        outside = max(0, before - p * PAIR)
        if outside:
            score = jnp.concatenate([score[:outside] + none_before, score[outside:]], axis=0)
        if p == pairs - 1:
            seen = SPAN - SEG
            score = jnp.concatenate([score[:seen] + jnp.where(q_row >= SEG, none_ahead, 0.0), score[seen:]], axis=0)
        top = jnp.max(score, axis=0, keepdims=True)
        expo = jnp.exp2(score - top)
        prob = expo / jnp.sum(expo, axis=0, keepdims=True)
        pgrad = dot(vb[rows, ls], g[cols, ls], ((1,), (1,)))
        delta = jnp.sum(prob * pgrad, axis=0, keepdims=True)
        sgrad = prob * (pgrad - delta)
        pt[h, rows, cols] = prob.astype(BF16)
        st[h, rows, cols] = (sgrad * scale).astype(BF16)
        if p == pairs - 1:
            acc[h] = sgrad
        else:
            acc[h] += sgrad

    def key_side(h, kblock, terms, other):
        p0, p1 = max(0, kblock - 2), min(pairs - 1, kblock)
        span = slice(p0 * PAIR, (p1 + 1) * PAIR)
        rows = slice(kblock * PAIR, (kblock + 1) * PAIR)
        return dot(terms[h, rows, span], other[span, lanes_of(h)], ((1,), (0,)))

    def bias_row(h):
        base = SEG * h
        far = acc[h, PAIR : 2 * PAIR]
        clipped = key_row < q_col
        rest = acc[h, 0:PAIR] + jnp.where(clipped, far, 0.0)
        rest = jnp.sum(jnp.sum(rest, axis=0, keepdims=True), axis=1, keepdims=True)
        x = jnp.concatenate([acc[h, 2 * PAIR : SPAN], jnp.where(clipped, 0.0, far)], axis=1)
        return diagonal_sums(x, SEG - 1 + base) + jnp.where(lane == base + BUCKETS - 1, rest, 0.0)

    def query_side(h, p):
        rows = slice(p * PAIR, p * PAIR + SPAN)
        return dot(st[h, rows, p * PAIR : (p + 1) * PAIR], kb[rows, lanes_of(h)], ((0,), (0,)))

    def give_back(h):
        ls = lanes_of(h)
        for terms, other, out, part, m in ((st, q, out_k, part_k, 0), (pt, g, out_v, part_v, 1)):
            out[0:PAIR, ls] = key_side(h, 0, terms, other).astype(BF16)
            edge = key_side(h, 1, terms, other)
            out[PAIR:before, ls] = edge[:SEG].astype(BF16)
            part[0:SEG, ls] = edge[SEG:]
            edge = key_side(h, 4, terms, other)
            part[SEG:PAIR, ls] = edge[:SEG]
            fwd[m, :, ls] = edge[SEG:].astype(BF16)
        edge = query_side(h, pairs - 1)
        dq_ref[0, tokens - SEG : tokens, ls] = edge[:SEG].astype(BF16)
        fwd[2, :, ls] = edge[SEG:].astype(BF16)
        n = 2 * h
        pieces = [
            send(o.at[:, lane_ds(h)], i.at[:, lane_ds(h)], back_send.at[n + a], back_recv.at[n + a], {"sp": prv})
            for a, (o, i) in enumerate(((out_k, in_k), (out_v, in_v)))
        ]
        n = 3 * h
        return pieces + [
            send(fwd.at[a, :, lane_ds(h)], got.at[a, :, lane_ds(h)], fwd_send.at[n + a], fwd_recv.at[n + a], {"sp": nxt})
            for a in range(3)
        ]

    hear(round_sem.at[0], heard)
    heard = greet(round_sem.at[1], steps((2, -2), "zy"))
    back = []
    rows_of = []
    for h in range(heads):
        for a in range(4):
            ahead[h, a].wait_recv()
        block(h, pairs - 1)
        for p in range(pairs - 2, -1, -1):
            if h and p == 0:
                rows_of.append(bias_row(h - 1))
                back += give_back(h - 1)
            for a in range(2):
                halo[h, a, p].wait_recv()
            block(h, p)
    rows_of.append(bias_row(heads - 1))
    hear(round_sem.at[1], heard)

    def spread(buf, axes, rows, ssem, rsem, values):
        moves = [m for m in itertools.product(*(range(sizes[a]) for a in axes)) if any(m)]
        moves.sort(key=lambda m: -sum(min(v, sizes[a] - v) for a, v in zip(axes, m)))

        def slot(m):
            n = 0
            for a, v in zip(axes, m):
                n = n * sizes[a] + lax.rem(here[a] + v, sizes[a])
            return n

        mine = slot((0,) * len(axes))
        for r, value in enumerate(values):
            buf[mine, r : r + 1, :] = value
        part = pl.ds(0, rows)
        for n, m in enumerate(moves):
            send(buf.at[mine, part], buf.at[mine, part], ssem.at[n], rsem.at[mine], at(**dict(zip(axes, m))))

        def collect():
            for m in reversed(moves):
                other = buf.at[slot(m), part]
                pltpu.make_async_remote_copy(
                    src_ref=other, dst_ref=other, send_sem=ssem.at[0], recv_sem=rsem.at[slot(m)],
                    device_id=at(), device_id_type=MESH,
                ).wait_recv()

        return collect

    first, second = rows_of
    collect = spread(
        bz, "zc", 3, z_send, z_recv,
        [first[:, :PAIR], first[:, PAIR:] + second[:, :PAIR], second[:, PAIR:]],
    )
    heard = greet(round_sem.at[2], steps((1, 2, 3), "x"))
    back += give_back(heads - 1)

    for h in range(heads):
        ls = lanes_of(h)
        for p in range(pairs - 1):
            dq_ref[0, SEG + p * PAIR : SEG + (p + 1) * PAIR, ls] = query_side(h, p).astype(BF16)
        for terms, other, out in ((st, q, dk_ref), (pt, g, dv_ref)):
            out[0, SEG : SEG + PAIR, ls] = key_side(h, 2, terms, other).astype(BF16)

    collect()
    values = []
    for c in range(2):
        total = bz[c, 0:3]
        for z in range(1, zs):
            total += bz[2 * z + c, 0:3]
        values += [total[r : r + 1] for r in range(3)]
    hear(round_sem.at[2], heard)
    early = len(sent)
    collect = spread(by, "yx", 6, y_send, y_recv, values)

    for h in range(heads):
        ls = lanes_of(h)
        for cp in back[5 * h : 5 * h + 5]:
            cp.wait_recv()
        dq_ref[0, 0:SEG, ls] = got[2, :, ls]
        for terms, other, out, part, come, m in ((st, q, dk_ref, part_k, in_k, 0), (pt, g, dv_ref, part_v, in_v, 1)):
            out[0, 0:SEG, ls] = (part[0:SEG, ls] + got[m, :, ls].astype(F32)).astype(BF16)
            mid = key_side(h, 3, terms, other) + come[0:PAIR, ls].astype(F32)
            out[0, tail : tail + PAIR, ls] = mid.astype(BF16)
            out[0, tokens - SEG : tokens, ls] = (part[SEG:PAIR, ls] + come[PAIR:before, ls].astype(F32)).astype(BF16)

    for cp in sent[:early]:
        cp.wait_send()
    collect()
    xs = tps // 2
    for x in range(xs):
        total = by[x, 0:6]
        for y in range(1, RING):
            total += by[y * xs + x, 0:6]
        for c in range(2):
            r = 2 * (2 * x + c)
            low, mid, high = (total[3 * c + n : 3 * c + n + 1] for n in range(3))
            db_ref[r : r + 1, :PAIR] = low
            db_ref[r : r + 1, PAIR:] = mid[:, : BUCKETS - PAIR]
            both = pltpu.roll(jnp.concatenate([mid, high], axis=1), 2 * PAIR - SEG, 1)
            db_ref[r + 1 : r + 2, :PAIR] = both[:, :PAIR]
            db_ref[r + 1 : r + 2, PAIR:] = both[:, PAIR:BUCKETS]
    for cp in sent[early:]:
        cp.wait_send()


def put_out(*refs):
    ins, outs, sem = refs[:4], refs[4:8], refs[8]
    copies = [pltpu.make_async_copy(i, o, sem.at[n]) for n, (i, o) in enumerate(zip(ins, outs))]
    for cp in copies:
        cp.start()
    for cp in copies:
        cp.wait()


def local(queries, keys, values, rel_bias, out_grad):
    _, tokens, width = queries.shape
    heads = width // HEAD_DIM
    tps = lax.axis_size("tp")
    zs = lax.axis_size("sp") // RING
    band = tokens + HALO
    dma = pltpu.SemaphoreType.DMA
    grad = jax.ShapeDtypeStruct(queries.shape, BF16)
    anywhere = pl.BlockSpec(memory_space=pl.ANY)
    vmem = pl.BlockSpec(memory_space=pltpu.VMEM)
    bias = jax.ShapeDtypeStruct((heads * tps, BUCKETS), F32)
    outs = (grad, grad, grad, bias)
    held = pl.pallas_call(
        functools.partial(body, tokens, heads),
        out_shape=tuple(pltpu.VMEM(o.shape, o.dtype) for o in outs),
        in_specs=[anywhere] * 5,
        out_specs=(vmem, vmem, vmem, vmem),
        scratch_shapes=[
            pltpu.VMEM((tokens, width), BF16),
            pltpu.VMEM((tokens, width), BF16),
            pltpu.VMEM((SEG, width), BF16),
            pltpu.VMEM((SEG, width), BF16),
            pltpu.VMEM((band, width), BF16),
            pltpu.VMEM((band, width), BF16),
            pltpu.VMEM((heads, band, tokens), BF16),
            pltpu.VMEM((heads, band, tokens), BF16),
            pltpu.VMEM((heads, SPAN, PAIR), F32),
            pltpu.VMEM((heads, SPAN, PAIR), F32),
            pltpu.VMEM((8, 2 * PAIR), F32),
            pltpu.VMEM((heads, BUCKETS), F32),
            pltpu.VMEM((HALO - SEG, width), BF16),
            pltpu.VMEM((HALO - SEG, width), BF16),
            pltpu.VMEM((HALO - SEG, width), BF16),
            pltpu.VMEM((HALO - SEG, width), BF16),
            pltpu.VMEM((3, SEG, width), BF16),
            pltpu.VMEM((3, SEG, width), BF16),
            pltpu.VMEM((PAIR, width), F32),
            pltpu.VMEM((PAIR, width), F32),
            pltpu.VMEM((RING * tps // 2, 8, PAIR), F32),
            pltpu.VMEM((zs * 2, 8, PAIR), F32),
            pltpu.SemaphoreType.REGULAR((3,)),
            dma((11,)),
            dma((4 * heads,)),
            dma((4 * heads,)),
            dma((4 * heads,)),
            dma((4 * heads,)),
            dma((2 * heads,)),
            dma((2 * heads,)),
            dma((3 * heads,)),
            dma((3 * heads,)),
            dma((RING * tps // 2,)),
            dma((RING * tps // 2,)),
            dma((zs * 2,)),
            dma((zs * 2,)),
        ],
        compiler_params=pltpu.CompilerParams(collective_id=0, has_side_effects=True),
    )(queries, keys, values, rel_bias, out_grad)
    return pl.pallas_call(
        put_out,
        out_shape=outs,
        in_specs=[vmem] * 4,
        out_specs=(anywhere,) * 4,
        scratch_shapes=[dma((4,))],
    )(*[pltpu.with_memory_space_constraint(x, pltpu.VMEM) for x in held])


def solution(mesh):
    return jax.shard_map(
        local,
        mesh=mesh,
        in_specs=(
            P(None, "sp", "tp"),
            P(None, "sp", "tp"),
            P(None, "sp", "tp"),
            P("tp", None),
            P(None, "sp", "tp"),
        ),
        out_specs=(P(None, "sp", "tp"), P(None, "sp", "tp"), P(None, "sp", "tp"), P()),
        check_vma=False,
    )
```
